128 devices in a mesh: fs: 16 (over z, y), tp: 8 (over x, core).
Axes of the slice: x: 4, y: 4, z: 4, core: 2. Of those that a mesh axis runs over, the one named last changes fastest.
Arguments:
- tokens: bfloat16 [16384, 2048], P(('fs', 'tp')), may hold values from -6 to 6
- first_block_norm_scale: float32 [2048], replicated, may hold values from 0.1 to 1.9
- first_block_gate_matrix: bfloat16 [2048, 5504], P('fs', 'tp'), may hold values from -0.125 to 0.125
- first_block_up_matrix: bfloat16 [2048, 5504], P('fs', 'tp'), may hold values from -0.125 to 0.125
- first_block_down_matrix: bfloat16 [5504, 2048], P('tp', 'fs'), may hold values from -0.078125 to 0.078125
- mixer_norm_scale: float32 [2048], replicated, may hold values from 0.1 to 1.9
- recurrent_input_matrix: bfloat16 [2048, 3072], P('fs', 'tp'), may hold values from -0.125 to 0.125
- output_gate_projection: bfloat16 [2048, 3072], P('fs', 'tp'), may hold values from -0.125 to 0.125
- convolution_kernel: float32 [4, 3072], P(None, 'tp'), may hold values from -2 to 2
- decay_gate_blocks: bfloat16 [16, 192, 192], P('tp'), may hold values from -0.4375 to 0.4375
- input_gate_blocks: bfloat16 [16, 192, 192], P('tp'), may hold values from -0.4375 to 0.4375
- channel_decay_weight: float32 [3072], P('tp'), may hold values from 3.5 to 11.5
- position_decay_extra: float32 [16384], P('fs'), may hold values from -0.7 to 0
- mixer_output_matrix: bfloat16 [3072, 2048], P('tp', 'fs'), may hold values from -0.109375 to 0.109375
- second_block_norm_scale: float32 [2048], replicated, may hold values from 0.1 to 1.9
- second_block_gate_matrix: bfloat16 [2048, 5504], P('fs', 'tp'), may hold values from -0.125 to 0.125
- second_block_up_matrix: bfloat16 [2048, 5504], P('fs', 'tp'), may hold values from -0.125 to 0.125
- second_block_down_matrix: bfloat16 [5504, 2048], P('tp', 'fs'), may hold values from -0.078125 to 0.078125
Outputs:
- layer_out: bfloat16 [16384, 2048], P(('fs', 'tp'))
The draws below stay inside these ranges and needn't reach their ends.
All inputs are finite; a program needn't handle non-finite values.
Results may differ from the reference program's by a relative error of at most 0.019.
Values may be sent and summed in bfloat16 or wider, within the bound.
A program may use at most 128 MiB of HBM per device.

```python
import jax
import jax.numpy as jnp
from jax import lax

D = 2048
FF = 5504
DR = 3072
RB = 16
BLK = 192
CONV = 4
SEQUENCE_TOKENS = 1024
TOKENS = 16384
N_TP = 8


def draw_channel_decay_weight(key, part):
    pick_key = jax.random.fold_in(key, 11)
    slow_key = jax.random.fold_in(key, 12)
    quick_key = jax.random.fold_in(key, 13)
    fraction = 0.5
    quick_mask = jax.random.bernoulli(pick_key, fraction, (DR,))
    slow_log = jax.random.uniform(slow_key, (DR,), jnp.float32, minval=jnp.log(2e-05), maxval=jnp.log(0.00025))
    quick_log = jax.random.uniform(quick_key, (DR,), jnp.float32, minval=jnp.log(0.004), maxval=jnp.log(0.02))
    softened = jnp.exp(jnp.where(quick_mask, quick_log, slow_log))
    return (-jnp.log(jnp.expm1(softened))).astype(jnp.float32)


def draw_position_decay_extra(key, part):
    where_key = jax.random.fold_in(key, 21)
    depth_key = jax.random.fold_in(key, 22)
    struck = jax.random.bernoulli(where_key, 4.0 / SEQUENCE_TOKENS, (TOKENS,))
    strength = jax.random.uniform(depth_key, (TOKENS,), jnp.float32, minval=jnp.log(0.5), maxval=jnp.log(0.8))
    return jnp.where(struck, strength, 0.0).astype(jnp.float32)


def block_scale(rng, dims, cuts, least, largest):
    def one(dim, parts):
        draws = jax.random.uniform(jax.random.fold_in(jax.random.fold_in(rng, 6), dim), (parts,), jnp.float32, least / len(cuts), largest / len(cuts))
        return jnp.repeat(jnp.exp(draws), dims[dim] // parts).reshape((-1,) + (1,) * (len(dims) - dim - 1))

    level = one(*cuts[0])
    for cut in cuts[1:]:
        level = level * one(*cut)
    return level


def centred(own_key, dims, spread, reach, cuts=(), dtype=jnp.bfloat16):
    loudness = block_scale(own_key, dims, cuts, -0.22, 0.18) if cuts else 1.0
    values = jax.random.normal(own_key, dims, jnp.float32) * spread * loudness
    return jnp.minimum(jnp.maximum(values, -reach), reach).astype(dtype)


def setup_inputs(seed: int = 0) -> dict:
    arg_keys = jax.random.split(jax.random.key(seed), 19)
    return {
        "tokens": centred(arg_keys[0], (TOKENS, D), 1.0, 6.0, ((0, 128),)),
        "first_block_norm_scale": jnp.clip(1.0 + 0.18 * jax.random.normal(arg_keys[1], (D,), jnp.float32), 0.1, 1.9),
        "first_block_gate_matrix": centred(arg_keys[2], (D, FF), D ** -0.5, 0.125, ((0, 16), (1, 8))),
        "first_block_up_matrix": centred(arg_keys[3], (D, FF), D ** -0.5, 0.125, ((0, 16), (1, 8))),
        "first_block_down_matrix": centred(arg_keys[4], (FF, D), FF ** -0.5, 0.078125, ((0, 8), (1, 16))),
        "mixer_norm_scale": jnp.clip(1.0 + 0.18 * jax.random.normal(arg_keys[5], (D,), jnp.float32), 0.1, 1.9),
        "recurrent_input_matrix": centred(arg_keys[6], (D, DR), D ** -0.5, 0.125, ((0, 16), (1, 8))),
        "output_gate_projection": centred(arg_keys[7], (D, DR), D ** -0.5, 0.125, ((0, 16), (1, 8))),
        "convolution_kernel": centred(arg_keys[8], (CONV, DR), 0.5, 2.0, ((1, 8),), jnp.float32),
        "decay_gate_blocks": centred(arg_keys[9], (RB, BLK, BLK), BLK ** -0.5, 0.4375, ((0, 8),)),
        "input_gate_blocks": centred(arg_keys[10], (RB, BLK, BLK), BLK ** -0.5, 0.4375, ((0, 8),)),
        "channel_decay_weight": draw_channel_decay_weight(jax.random.fold_in(arg_keys[18], 71), 0),
        "position_decay_extra": draw_position_decay_extra(jax.random.fold_in(arg_keys[18], 71), 0),
        "mixer_output_matrix": centred(arg_keys[13], (DR, D), DR ** -0.5, 0.109375, ((0, 8), (1, 16))),
        "second_block_norm_scale": jnp.clip(1.0 + 0.18 * jax.random.normal(arg_keys[14], (D,), jnp.float32), 0.1, 1.9),
        "second_block_gate_matrix": centred(arg_keys[15], (D, FF), D ** -0.5, 0.125, ((0, 16), (1, 8))),
        "second_block_up_matrix": centred(arg_keys[16], (D, FF), D ** -0.5, 0.125, ((0, 16), (1, 8))),
        "second_block_down_matrix": centred(arg_keys[17], (FF, D), FF ** -0.5, 0.078125, ((0, 8), (1, 16))),
    }


EPS = 1e-06
RECURRENT_WIDTH = 8.0

def normed(input_token_rows, norm_scale_vector):
    values = input_token_rows.astype(jnp.float32)
    square = lax.optimization_barrier(jnp.mean(values * values, axis=-1, keepdims=True))
    return (values * lax.rsqrt(square + EPS) * norm_scale_vector).astype(jnp.bfloat16)

def block_sum(hidden, weight):
    span_width = hidden.shape[1] // N_TP
    running = jnp.zeros((hidden.shape[0], weight.shape[1]), jnp.float32)
    for index_k in range(N_TP):
        lower = index_k * span_width
        partial_sum = jnp.dot(hidden[:, lower:lower + span_width], weight[lower:lower + span_width], preferred_element_type=jnp.float32).astype(jnp.bfloat16)
        partial_sum = lax.optimization_barrier(partial_sum)
        running = running + partial_sum.astype(jnp.float32)
    return running

def feed_forward(input_token_rows, norm_scale_vector, gate_weight, up_weight, down_weight):
    normal = normed(input_token_rows, norm_scale_vector)
    gate_pre = jnp.dot(normal, gate_weight, preferred_element_type=jnp.float32)
    up_pre = jnp.dot(normal, up_weight, preferred_element_type=jnp.float32)
    hidden = (jax.nn.silu(gate_pre) * up_pre).astype(jnp.bfloat16)
    return block_sum(hidden, down_weight)

def blockwise(values, weight):
    dims_in = values.shape
    grouped = values.reshape(dims_in[:-1] + (weight.shape[0], weight.shape[1])).astype(jnp.float32)
    result = jnp.einsum('sthi,hij->sthj', grouped, weight.astype(jnp.float32))
    return result.reshape(dims_in)

def combine(earlier, later):
    decay_one, drive_one = earlier
    decay_two, drive_two = later
    return (decay_one * decay_two, decay_two * drive_one + drive_two)

def linear_recurrence_scan(input_token_rows, norm_scale_vector, recurrent_input_matrix, output_gate_projection, convolution_kernel, decay_gate_blocks, input_gate_blocks, channel_decay_weight, position_decay_extra, mixer_output_matrix):
    normal = normed(input_token_rows, norm_scale_vector)
    sequence_batch_count = normal.shape[0] // SEQUENCE_TOKENS
    recur_rows = jnp.dot(normal, recurrent_input_matrix, preferred_element_type=jnp.float32).astype(jnp.bfloat16)
    branch_rows = jnp.dot(normal, output_gate_projection, preferred_element_type=jnp.float32).astype(jnp.bfloat16)
    recur_rows = recur_rows.reshape(sequence_batch_count, SEQUENCE_TOKENS, -1)
    branch_rows = branch_rows.reshape(sequence_batch_count, SEQUENCE_TOKENS, -1)
    taps = convolution_kernel.shape[0]
    padded = jnp.pad(recur_rows, ((0, 0), (taps - 1, 0), (0, 0)))
    summed = jnp.zeros(recur_rows.shape, jnp.float32)
    for offset in range(taps):
        summed = summed + padded[:, offset:offset + SEQUENCE_TOKENS].astype(jnp.float32) * convolution_kernel[offset]
    conv_out = summed.astype(jnp.bfloat16)
    decay_gate_value = jax.nn.sigmoid(blockwise(conv_out, decay_gate_blocks))
    input_gate = jax.nn.sigmoid(blockwise(conv_out, input_gate_blocks))
    log_decay_factor = -RECURRENT_WIDTH * decay_gate_value * jax.nn.softplus(-channel_decay_weight) + position_decay_extra.reshape(sequence_batch_count, SEQUENCE_TOKENS, 1)
    decay_rate = jnp.exp(log_decay_factor)
    drive_in = jnp.sqrt(-jnp.expm1(2.0 * log_decay_factor)) * input_gate * conv_out.astype(jnp.float32)
    _, hidden_state = lax.associative_scan(combine, (decay_rate, drive_in), axis=1)
    gated = (jax.nn.gelu(branch_rows.astype(jnp.float32), approximate=True) * hidden_state).astype(jnp.bfloat16)
    return block_sum(gated.reshape(sequence_batch_count * SEQUENCE_TOKENS, -1), mixer_output_matrix)

def reference(tokens, first_block_norm_scale, first_block_gate_matrix, first_block_up_matrix, first_block_down_matrix, mixer_norm_scale, recurrent_input_matrix, output_gate_projection, convolution_kernel, decay_gate_blocks, input_gate_blocks, channel_decay_weight, position_decay_extra, mixer_output_matrix, second_block_norm_scale, second_block_gate_matrix, second_block_up_matrix, second_block_down_matrix):
    first_out = feed_forward(tokens, first_block_norm_scale, first_block_gate_matrix, first_block_up_matrix, first_block_down_matrix)
    residual_activations = (tokens.astype(jnp.float32) + 0.5 * first_out).astype(jnp.bfloat16)
    mixer_output_rows = linear_recurrence_scan(residual_activations, mixer_norm_scale, recurrent_input_matrix, output_gate_projection, convolution_kernel, decay_gate_blocks, input_gate_blocks, channel_decay_weight, position_decay_extra, mixer_output_matrix)
    residual_activations = (residual_activations.astype(jnp.float32) + mixer_output_rows).astype(jnp.bfloat16)
    second_out = feed_forward(residual_activations, second_block_norm_scale, second_block_gate_matrix, second_block_up_matrix, second_block_down_matrix)
    return (residual_activations.astype(jnp.float32) + 0.5 * second_out).astype(jnp.bfloat16)
```

```python
import functools

import jax
import jax.numpy as jnp
from jax import lax
from jax.experimental import pallas as pl
from jax.experimental.pallas import tpu as pltpu
from jax.sharding import PartitionSpec as P

EPS = 1e-06
MESH = pl.DeviceIdType.MESH
F32 = jnp.float32
BF16 = jnp.bfloat16

ROWS = 128
HALF = ROWS // 2
D = 2048
NFS = 16
HID = 688
HPAD = 768
CH = 384
SEQ = 1024
FULL_TILES = HID // 128
FFN_ROWS = HID + 2 * FULL_TILES * 128 + 128
MIX_ROWS = 3 * CH
FFN_CUTS = (0, 528, 1056, 1584, 2096)
MIX_CUTS = (0, 288, 576, 864, 1152)


def sigmoid(v):
    return 1.0 / (1.0 + jnp.exp(-v))


def one_minus_exp(v):
    series = 1.0 / 720.0 + v * (1.0 / 5040.0)
    for term in (1.0 / 120.0, 1.0 / 24.0, 1.0 / 6.0, 0.5, 1.0):
        series = term + v * series
    return jnp.where(v > -0.3, -v * series, 1.0 - jnp.exp(v))


def layer_kernel(
    tok, s1, s2, s3,
    g1, u1, t1, d1, ri, og, mo, g3, u3, t3, d3,
    ck, gb, cv, pde,
    out,
    w1, w2, w3, xg, hid, ps, pr, po, sb, rb, res, rc, br, sa, sd,
    wl, ws, wr, ags, agr, prs, prr, rss, rsr,
):
    fs = lax.axis_index("fs")
    tp = lax.axis_index("tp")
    z, y = fs // 4, fs % 4
    x, c = tp // 2, tp % 2

    def chip(dx):
        return (x + dx) % 4

    def dev_x(dx):
        return (fs, chip(dx) * 2 + c)

    partner = (fs, x * 2 + (1 - c))
    right, left = dev_x(1), dev_x(3)

    def fs_of(dz, dy):
        return ((z + dz) % 4) * 4 + (y + dy) % 4

    def rcopy(src, dst, ssem, rsem, dev):
        return pltpu.make_async_remote_copy(
            src_ref=src, dst_ref=dst, send_sem=ssem, recv_sem=rsem,
            device_id=dev, device_id_type=MESH,
        )

    def load_ffn(w, g, u, t, d, sem):
        pltpu.make_async_copy(d, w.at[fs, pl.ds(0, HID)], sem).start()
        for j in range(FULL_TILES):
            cols = pl.ds(j * 128, 128)
            pltpu.make_async_copy(g.at[:, cols], w.at[fs, pl.ds(HID + j * 128, 128)], sem).start()
            pltpu.make_async_copy(
                u.at[:, cols], w.at[fs, pl.ds(HID + (FULL_TILES + j) * 128, 128)], sem
            ).start()
        pltpu.make_async_copy(t, w.at[fs, pl.ds(HID + 2 * FULL_TILES * 128, 128)], sem).start()

    def load_mix(w, sem):
        pltpu.make_async_copy(mo, w.at[fs, pl.ds(0, CH)], sem).start()
        for j in range(CH // 128):
            cols = pl.ds(j * 128, 128)
            pltpu.make_async_copy(ri.at[:, cols], w.at[fs, pl.ds(CH + j * 128, 128)], sem).start()
            pltpu.make_async_copy(og.at[:, cols], w.at[fs, pl.ds(2 * CH + j * 128, 128)], sem).start()

    def wait_load(w, sem):
        pltpu.make_async_copy(w.at[fs], w.at[fs], sem).wait()

    def weight_steps(n, w, cuts):
        def block(h, dp, dq):
            return fs_of(dq, dp) if h == 0 else fs_of(dp, dq)

        def rows(h, part):
            lo, mid, hi = cuts[2 * h], cuts[2 * h + 1], cuts[2 * h + 2]
            a, b = {"all": (lo, hi), "first": (lo, mid), "second": (mid, hi)}[part]
            return pl.ds(a, b - a)

        started = []

        def desc(h, dp, dq, part, k, to):
            ref = w.at[block(h, dp, dq), rows(h, part)]
            return rcopy(ref, ref, ws.at[n, 20 * h + k], wr.at[n, 20 * h + k], (block(h, *to), tp))

        def send(*a):
            cp = desc(*a)
            cp.start()
            started.append(cp)

        def recv(h, dp, dq, part, k):
            desc(h, dp, dq, part, k, (0, 0)).wait_recv()

        offs = (0, 3, 1, 2)

        def start():
            for h in (0, 1):
                send(h, 0, 0, "all", 0, (1, 0))
                send(h, 0, 0, "all", 1, (3, 0))
            for h in (0, 1):
                send(h, 0, 0, "all", 4, (0, 1))
                send(h, 0, 0, "all", 5, (0, 3))

        def across(h, j):
            send(h, offs[j], 0, "all", 4 + 4 * j, (0, 1))
            send(h, offs[j], 0, "all", 5 + 4 * j, (0, 3))

        def near(j):
            for h in (0, 1):
                recv(h, offs[j], 0, "all", j - 1)
                if j == 1:
                    send(h, 3, 0, "first", 2, (1, 0))
                else:
                    send(h, 1, 0, "second", 3, (3, 0))
            for h in (0, 1):
                across(h, j)

        def far():
            for h in (0, 1):
                recv(h, 2, 0, "first", 2)
                recv(h, 2, 0, "second", 3)
                across(h, 3)

        def forward(j):
            for h in (0, 1):
                recv(h, offs[j], 3, "all", 4 + 4 * j)
                send(h, offs[j], 3, "first", 6 + 4 * j, (0, 1))
            for h in (0, 1):
                recv(h, offs[j], 1, "all", 5 + 4 * j)
                send(h, offs[j], 1, "second", 7 + 4 * j, (0, 3))

        def last():
            for j in range(4):
                for h in (0, 1):
                    recv(h, offs[j], 2, "first", 6 + 4 * j)
                    recv(h, offs[j], 2, "second", 7 + 4 * j)

        def drain():
            for cp in started:
                cp.wait_send()

        return [
            start,
            functools.partial(near, 1),
            functools.partial(near, 2),
            functools.partial(forward, 0),
            far,
            functools.partial(forward, 1),
            functools.partial(forward, 2),
            functools.partial(forward, 3),
            last,
            drain,
        ]

    def gather_steps(l):
        lo, hi = pl.ds(0, HALF), pl.ds(HALF, HALF)
        started = []

        def blk(dx, same=True):
            return chip(dx) * 2 + (c if same else 1 - c)

        def send(ref, k, dev):
            cp = rcopy(ref, ref, ags.at[l, k], agr.at[l, k], dev)
            cp.start()
            started.append(cp)

        def recv(ref, k):
            rcopy(ref, ref, ags.at[l, k], agr.at[l, k], partner).wait_recv()

        def start():
            mine = xg.at[blk(0)]
            send(xg.at[blk(0), lo], 1, right)
            send(xg.at[blk(0), hi], 2, left)
            send(xg.at[blk(0), hi], 3, right)
            send(xg.at[blk(0), lo], 4, left)
            send(mine, 0, partner)

        def forward():
            recv(xg.at[blk(3), lo], 1)
            send(xg.at[blk(3), lo], 5, right)
            recv(xg.at[blk(1), hi], 2)
            send(xg.at[blk(1), hi], 6, left)

        def near():
            recv(xg.at[blk(3), hi], 3)
            send(xg.at[blk(3)], 7, partner)
            recv(xg.at[blk(1), lo], 4)
            send(xg.at[blk(1)], 8, partner)

        def far():
            recv(xg.at[blk(2), lo], 5)
            recv(xg.at[blk(2), hi], 6)
            send(xg.at[blk(2)], 9, partner)

        def ready(dx):
            recv(xg.at[blk(dx, False)], {0: 0, 3: 7, 1: 8, 2: 9}[dx])

        def drain():
            for cp in started:
                cp.wait_send()

        return start, forward, near, far, ready, drain

    def normed(values, scale):
        square = jnp.mean(values * values, axis=-1, keepdims=True)
        return (values * lax.rsqrt(square + EPS) * scale[...]).astype(BF16)

    G = 16

    def first_norm():
        def body(i, _):
            r = pl.ds(pl.multiple_of(i * G, G), G)
            xg[tp, r, :] = normed(tok[r, :].astype(F32), s1)
            return 0

        lax.fori_loop(0, ROWS // G, body, 0)

    def ffn_in(w, dx):
        xd = chip(dx)
        lhs = xg[pl.ds(2 * xd, 2)].reshape(2 * ROWS, D)

        def tile(at):
            return w[:, pl.ds(pl.multiple_of(at, 16), 128), :].reshape(D, 128)

        def body(j, _):
            rhs = jnp.concatenate([tile(HID + j * 128), tile(HID + (FULL_TILES + j) * 128)], axis=1)
            r = jnp.dot(lhs, rhs, preferred_element_type=F32)
            g, u = r[:, :128], r[:, 128:]
            h = (g * sigmoid(g) * u).astype(BF16)
            hid[pl.ds(2 * xd, 2), :, pl.ds(pl.multiple_of(j * 128, 128), 128)] = h.reshape(2, ROWS, 128)
            return 0

        lax.fori_loop(0, FULL_TILES, body, 0)
        r = jnp.dot(lhs, tile(HID + 2 * FULL_TILES * 128), preferred_element_type=F32)
        u = pltpu.roll(r, 128 - (HID - FULL_TILES * 128), 1)
        lane = lax.broadcasted_iota(jnp.int32, r.shape, 1)
        h = jnp.where(lane < HID - FULL_TILES * 128, r * sigmoid(r) * u, 0.0).astype(BF16)
        hid[pl.ds(2 * xd, 2), :, pl.ds(FULL_TILES * 128, 128)] = h.reshape(2, ROWS, 128)

    def mix_in(dx):
        xd = chip(dx)
        lhs = xg[pl.ds(2 * xd, 2)].reshape(2 * ROWS, D)

        def tile(at):
            return w2[:, pl.ds(pl.multiple_of(at, 16), 128), :].reshape(D, 128)

        def body(j, _):
            rhs = jnp.concatenate([tile(CH + j * 128), tile(2 * CH + j * 128)], axis=1)
            r = jnp.dot(lhs, rhs, preferred_element_type=F32).astype(BF16)
            cols = pl.ds(pl.multiple_of(j * 128, 128), 128)
            rc[pl.ds(pl.multiple_of(8 + xd * 256, 8), 256), cols] = r[:, :128].astype(F32)
            br[pl.ds(pl.multiple_of(xd * 256, 256), 256), cols] = r[:, 128:]
            return 0

        lax.fori_loop(0, CH // 128, body, 0)

    def gates(i):
        at = pl.multiple_of(i * 256, 256)
        tiles = []
        for j in range(CH // 128):
            cols = pl.ds(j * 128, 128)
            window = rc[pl.ds(at, 264), cols]
            acc = window[8:] * ck[3:4, cols]
            for s in (1, 2, 3):
                acc = acc + pltpu.roll(window, s, 0)[8:] * ck[3 - s : 4 - s, cols]
            tiles.append(acc.astype(BF16))
        conv = jnp.concatenate(tiles, axis=1)
        both = jnp.dot(conv, gb[...], preferred_element_type=F32)
        extra = pde[pl.ds(at, 256), :]
        for j in range(CH // 128):
            cols = pl.ds(j * 128, 128)
            rate = sigmoid(both[:, j * 128 : (j + 1) * 128])
            gate = sigmoid(both[:, CH + j * 128 : CH + (j + 1) * 128])
            log_a = rate * cv[:, cols] + extra
            sa[pl.ds(at, 256), cols] = jnp.exp(log_a)
            sd[pl.ds(at, 256), cols] = (
                jnp.sqrt(one_minus_exp(2.0 * log_a)) * gate * tiles[j].astype(F32)
            )

    T = 64

    def scan_chunk(i, carry):
        r = pl.ds(pl.multiple_of(i * T, T), T)
        a, b = sa[r, :], sd[r, :]
        row = lax.broadcasted_iota(jnp.int32, (T, CH), 0)
        s = 1
        while s < T:
            here = row >= s
            b = a * jnp.where(here, pltpu.roll(b, s, 0), 0.0) + b
            a = a * jnp.where(here, pltpu.roll(a, s, 0), 1.0)
            s *= 2
        state = b + a * carry
        v = br[r, :].astype(F32)
        gelu = 0.5 * v * (1.0 + jnp.tanh(0.7978845608028654 * (v + 0.044715 * v * v * v)))
        hid[i // 2, pl.ds(pl.multiple_of((i % 2) * T, T), T), pl.ds(0, CH)] = (gelu * state).astype(BF16)
        return state[T - 1 : T, :]

    SLOT = {2: 0, 1: 1, 3: 2, 0: 3}

    def project(l, w, depth, dx):
        xd = chip(dx)
        k = SLOT[dx]
        lhs = jnp.concatenate(
            [hid[2 * xd + 1 - c, :, pl.ds(0, depth)], hid[2 * xd + c, :, pl.ds(0, depth)]], axis=0
        )

        def body(n, _):
            rhs = jnp.concatenate([w[2 * n, pl.ds(0, depth), :], w[2 * n + 1, pl.ds(0, depth), :]], axis=1)
            r = jnp.dot(lhs, rhs, preferred_element_type=F32).astype(BF16)
            cols = pl.ds(pl.multiple_of(n * 256, 256), 256)
            ps[k, :, cols] = r[:ROWS]
            po[k, :, cols] = r[ROWS:]
            return 0

        lax.fori_loop(0, NFS // 2, body, 0)
        rcopy(ps.at[k], pr.at[k], prs.at[l, k], prr.at[l, k], partner).start()

    def pair_ready(l, dx):
        k = SLOT[dx]
        rcopy(ps.at[k], pr.at[k], prs.at[l, k], prr.at[l, k], partner).wait_recv()

    def pair(k, r):
        return po[k, r, :].astype(F32) + pr[k, r, :].astype(F32)

    def ring(l, way, slot):
        return rcopy(
            sb.at[way, slot], rb.at[way, slot], rss.at[l, way, slot], rsr.at[l, way, slot],
            (right, left)[way],
        )

    def post(l, way, slot, dx, base, extra=None):
        def body(i, _):
            at = pl.multiple_of(i * G, G)
            v = pair(SLOT[dx], pl.ds(base + at, G))
            if extra is not None:
                v = v + rb[way, extra, pl.ds(at, G), :].astype(F32)
            sb[way, slot, pl.ds(at, G), :] = v.astype(BF16)
            return 0

        lax.fori_loop(0, HALF // G, body, 0)
        ring(l, way, slot).start()

    def finish(l, before, weight, scale, result):
        ring(l, 0, 2).wait_recv()
        ring(l, 1, 1).wait_recv()
        for base, a, b in ((0, 2, 1), (HALF, 1, 2)):
            if base:
                ring(l, 0, 1).wait_recv()
                ring(l, 1, 2).wait_recv()

            def body(i, _):
                at = pl.multiple_of(i * G, G)
                r = pl.ds(base + at, G)
                v = pair(SLOT[0], r)
                v = v + rb[0, a, pl.ds(at, G), :].astype(F32) + rb[1, b, pl.ds(at, G), :].astype(F32)
                v = (before[r, :].astype(F32) + weight * v).astype(BF16)
                result[r, :] = v
                if scale is not None:
                    xg[tp, r, :] = normed(v.astype(F32), scale)
                return 0

            lax.fori_loop(0, HALF // G, body, 0)

    def reduce(l, w, depth, before, weight, scale, result, steps):
        steps = iter(steps)

        def step():
            for s in next(steps, ()):
                s()

        project(l, w, depth, 2)
        step()
        project(l, w, depth, 1)
        pair_ready(l, 2)
        post(l, 0, 0, 2, 0)
        post(l, 1, 0, 2, HALF)
        step()
        project(l, w, depth, 3)
        pair_ready(l, 1)
        post(l, 0, 1, 1, HALF)
        project(l, w, depth, 0)
        pair_ready(l, 3)
        post(l, 1, 1, 3, 0)
        step()
        ring(l, 0, 0).wait_recv()
        post(l, 0, 2, 1, 0, extra=0)
        ring(l, 1, 0).wait_recv()
        post(l, 1, 2, 3, HALF, extra=0)
        step()
        pair_ready(l, 0)
        finish(l, before, weight, scale, result)
        for k in range(4):
            rcopy(ps.at[k], pr.at[k], prs.at[l, k], prr.at[l, k], partner).wait_send()
        for way in (0, 1):
            for slot in range(3):
                ring(l, way, slot).wait_send()

    load_ffn(w1, g1, u1, t1, d1, wl.at[0])
    load_mix(w2, wl.at[1])
    load_ffn(w3, g3, u3, t3, d3, wl.at[2])

    barrier = pltpu.get_barrier_semaphore()
    peers = [right, left, partner] + [(fs_of(*d), tp) for d in ((0, 1), (0, 3), (1, 0), (3, 0))]
    for dev in peers:
        pl.semaphore_signal(barrier, inc=1, device_id=dev, device_id_type=MESH)
    first_norm()
    rc[pl.ds(0, 8), :] = jnp.zeros((8, CH), F32)
    pl.semaphore_wait(barrier, len(peers))

    a1 = weight_steps(0, w1, FFN_CUTS)
    a2 = weight_steps(1, w2, MIX_CUTS)
    a3 = weight_steps(2, w3, FFN_CUTS)

    wait_load(w1, wl.at[0])
    a1[0]()
    start, forward, near, far, ready, drain = gather_steps(0)
    start()
    a1[1]()
    a1[2]()
    forward()
    a1[3]()
    near()
    a1[4]()
    far()
    a1[5]()
    for dx in (0, 3, 1, 2):
        ready(dx)
    drain()
    wait_load(w2, wl.at[1])
    wait_load(w3, wl.at[2])
    a1[6]()
    a1[7]()
    a2[0]()
    a1[8]()
    for i, dx in enumerate((2, 1, 3, 0)):
        ffn_in(w1, dx)
        if i == 1:
            a2[1]()
        if i == 2:
            a2[2]()
        if i == 3:
            a2[3]()
    reduce(0, w1, HPAD, tok, 0.5, s2, res, [[a2[4]], [a2[5]], [a2[6]], [a2[7], a3[0]]])

    start, forward, near, far, ready, drain = gather_steps(1)
    start()
    a2[8]()
    ready(0)
    mix_in(0)
    forward()
    a3[1]()
    near()
    a3[2]()
    ready(3)
    mix_in(3)
    ready(1)
    mix_in(1)
    far()
    a3[3]()
    ready(2)
    mix_in(2)
    drain()
    a3[4]()

    def gate_body(i, _):
        gates(i)
        return 0

    lax.fori_loop(0, SEQ // 256, gate_body, 0)
    a3[5]()
    lax.fori_loop(0, SEQ // T, scan_chunk, jnp.zeros((1, CH), F32))
    reduce(1, w2, CH, res, 1.0, s3, res, [[a3[6]], [], [a3[7]], []])

    start, forward, near, far, ready, drain = gather_steps(2)
    start()
    a3[8]()
    ready(0)
    ffn_in(w3, 0)
    forward()
    near()
    ready(3)
    ffn_in(w3, 3)
    ready(1)
    ffn_in(w3, 1)
    far()
    ready(2)
    ffn_in(w3, 2)
    drain()
    reduce(2, w3, HPAD, res, 0.5, None, out, [])
    a1[9]()
    a2[9]()
    a3[9]()


def gate_map(decay, inputs):
    def diagonal(b):
        return jnp.concatenate(
            [jnp.pad(b[0], ((0, 0), (0, 192))), jnp.pad(b[1], ((0, 0), (192, 0)))], axis=0
        )

    return jnp.concatenate([diagonal(decay), diagonal(inputs)], axis=1)


def tail(gate, up):
    at = FULL_TILES * 128
    left = gate.shape[1] - at
    return jnp.concatenate(
        [gate[:, at:], up[:, at:], jnp.zeros((gate.shape[0], 128 - 2 * left), gate.dtype)], axis=1
    )


def shards(
    tokens, s1, g1, u1, d1, s2, ri, og, ck, decay, inputs, cdw, extra, mo, s3, g3, u3, d3
):
    vmem = pl.BlockSpec(memory_space=pltpu.VMEM)
    hbm = pl.BlockSpec(memory_space=pl.ANY)
    row = lambda v: v.reshape(1, -1)
    dma = pltpu.SemaphoreType.DMA
    return pl.pallas_call(
        layer_kernel,
        out_shape=jax.ShapeDtypeStruct((ROWS, D), BF16),
        in_specs=[vmem] * 4 + [hbm] * 11 + [vmem] * 4,
        out_specs=vmem,
        scratch_shapes=[
            pltpu.VMEM((NFS, FFN_ROWS, 128), BF16),
            pltpu.VMEM((NFS, MIX_ROWS, 128), BF16),
            pltpu.VMEM((NFS, FFN_ROWS, 128), BF16),
            pltpu.VMEM((8, ROWS, D), BF16),
            pltpu.VMEM((8, ROWS, HPAD), BF16),
            pltpu.VMEM((4, ROWS, D), BF16),
            pltpu.VMEM((4, ROWS, D), BF16),
            pltpu.VMEM((4, ROWS, D), BF16),
            pltpu.VMEM((2, 3, HALF, D), BF16),
            pltpu.VMEM((2, 3, HALF, D), BF16),
            pltpu.VMEM((ROWS, D), BF16),
            pltpu.VMEM((SEQ + 8, CH), F32),
            pltpu.VMEM((SEQ, CH), BF16),
            pltpu.VMEM((SEQ, CH), F32),
            pltpu.VMEM((SEQ, CH), F32),
            dma((3,)),
            dma((3, 40)),
            dma((3, 40)),
            dma((3, 10)),
            dma((3, 10)),
            dma((3, 4)),
            dma((3, 4)),
            dma((3, 2, 3)),
            dma((3, 2, 3)),
        ],
        compiler_params=pltpu.CompilerParams(
            collective_id=0, has_side_effects=True, vmem_limit_bytes=60 * 1024 * 1024
        ),
        name="layer",
    )(
        tokens, row(s1), row(s2), row(s3),
        g1, u1, tail(g1, u1), d1, ri, og, mo, g3, u3, tail(g3, u3), d3,
        ck, gate_map(decay, inputs), row(-8.0 * jax.nn.softplus(-cdw)),
        jnp.broadcast_to(extra[:, None], (SEQ, 128)),
    )


def solution(mesh):
    in_specs = (
        P(("fs", "tp"), None), P(), P("fs", "tp"), P("fs", "tp"), P("tp", "fs"),
        P(), P("fs", "tp"), P("fs", "tp"), P(None, "tp"), P("tp", None, None),
        P("tp", None, None), P("tp"), P("fs"), P("tp", "fs"), P(),
        P("fs", "tp"), P("fs", "tp"), P("tp", "fs"),
    )
    out_specs = P(("fs", "tp"), None)
    return jax.shard_map(shards, mesh=mesh, in_specs=in_specs, out_specs=out_specs, check_vma=False)
```

```python
import functools

import jax
import jax.numpy as jnp
from jax import lax
from jax.experimental import pallas as pl
from jax.experimental.pallas import tpu as pltpu
from jax.sharding import PartitionSpec as P

EPS = 1e-06
MESH = pl.DeviceIdType.MESH
F32 = jnp.float32
BF16 = jnp.bfloat16

ROWS = 128
HALF = ROWS // 2
D = 2048
NFS = 16
HID = 688
HPAD = 768
BLK = 192
CH = 384
SEQ = 1024
FULL_TILES = HID // 128
FFN_ROWS = HID + 2 * FULL_TILES * 128 + 128
MIX_ROWS = 3 * CH
FFN_CUTS = (0, 528, 1056, 1584, 2096)
IN_CUTS = (688, 1040, 1392, 1744, 2096)
DOWN_CUTS = (0, 176, 352, 528, 688)
MIX_CUTS = (0, 288, 576, 864, 1152)


def sigmoid(v):
    return 1.0 / (1.0 + jnp.exp(-v))


def one_minus_exp(v):
    series = 1.0 / 720.0 + v * (1.0 / 5040.0)
    for term in (1.0 / 120.0, 1.0 / 24.0, 1.0 / 6.0, 0.5, 1.0):
        series = term + v * series
    return jnp.where(v > -0.3, -v * series, 1.0 - jnp.exp(v))


def layer_kernel(
    tok, s1, s2, s3,
    g1, u1, g3, u3, ck, decay, inputs, cdw, extra,
    d1, ri, og, mo, d3,
    out,
    w1, w2, w3, xg, hid, ps, pr, po, sb, rb, res, rc, br, sa, sd, gb,
    wl, ws, wr, ags, agr, prs, prr, rss, rsr,
):
    fs = lax.axis_index("fs")
    tp = lax.axis_index("tp")
    z, y = fs // 4, fs % 4
    x, c = tp // 2, tp % 2

    def chip(dx):
        return (x + dx) % 4

    def dev_x(dx):
        return (fs, chip(dx) * 2 + c)

    partner = (fs, x * 2 + (1 - c))
    right, left = dev_x(1), dev_x(3)

    def fs_of(dz, dy):
        return ((z + dz) % 4) * 4 + (y + dy) % 4

    def rcopy(src, dst, ssem, rsem, dev):
        return pltpu.make_async_remote_copy(
            src_ref=src, dst_ref=dst, send_sem=ssem, recv_sem=rsem,
            device_id=dev, device_id_type=MESH,
        )

    def load_ffn(w, g, u, d, sem):
        pltpu.make_async_copy(d, w.at[fs, pl.ds(0, HID)], sem).start()
        for j in range(FULL_TILES):
            rows = pl.ds(j * 128, 128)
            w[fs, pl.ds(HID + j * 128, 128), :] = g[rows, :].T
            w[fs, pl.ds(HID + (FULL_TILES + j) * 128, 128), :] = u[rows, :].T
        at = FULL_TILES * 128
        last = jnp.concatenate(
            [g[at:HID, :], u[at:HID, :], jnp.zeros((128 - 2 * (HID - at), 128), BF16)], axis=0
        )
        w[fs, pl.ds(HID + 2 * at, 128), :] = last.T

    def wait_ffn(w, d, sem):
        pltpu.make_async_copy(d, w.at[fs, pl.ds(0, HID)], sem).wait()

    def load_mix(w, sem):
        pltpu.make_async_copy(mo, w.at[fs, pl.ds(0, CH)], sem).start()
        for j in range(CH // 128):
            cols = pl.ds(j * 128, 128)
            pltpu.make_async_copy(ri.at[:, cols], w.at[fs, pl.ds(CH + j * 128, 128)], sem).start()
            pltpu.make_async_copy(og.at[:, cols], w.at[fs, pl.ds(2 * CH + j * 128, 128)], sem).start()

    def wait_load(w, sem):
        pltpu.make_async_copy(w.at[fs], w.at[fs], sem).wait()

    def weight_steps(n, w, cuts):
        def block(h, dp, dq):
            return fs_of(dq, dp) if h == 0 else fs_of(dp, dq)

        def rows(h, part):
            lo, mid, hi = cuts[2 * h], cuts[2 * h + 1], cuts[2 * h + 2]
            a, b = {"all": (lo, hi), "first": (lo, mid), "second": (mid, hi)}[part]
            return pl.ds(a, b - a)

        started = []

        def desc(h, dp, dq, part, k, to):
            ref = w.at[block(h, dp, dq), rows(h, part)]
            return rcopy(ref, ref, ws.at[n, 20 * h + k], wr.at[n, 20 * h + k], (block(h, *to), tp))

        def send(*a):
            cp = desc(*a)
            cp.start()
            started.append(cp)

        def recv(h, dp, dq, part, k):
            desc(h, dp, dq, part, k, (0, 0)).wait_recv()

        offs = (0, 3, 1, 2)

        def start():
            for h in (0, 1):
                send(h, 0, 0, "all", 0, (1, 0))
                send(h, 0, 0, "all", 1, (3, 0))
            for h in (0, 1):
                send(h, 0, 0, "all", 4, (0, 1))
                send(h, 0, 0, "all", 5, (0, 3))

        def across(h, j):
            send(h, offs[j], 0, "all", 4 + 4 * j, (0, 1))
            send(h, offs[j], 0, "all", 5 + 4 * j, (0, 3))

        def near(j):
            for h in (0, 1):
                recv(h, offs[j], 0, "all", j - 1)
                if j == 1:
                    send(h, 3, 0, "first", 2, (1, 0))
                else:
                    send(h, 1, 0, "second", 3, (3, 0))
            for h in (0, 1):
                across(h, j)

        def far():
            for h in (0, 1):
                recv(h, 2, 0, "first", 2)
                recv(h, 2, 0, "second", 3)
                across(h, 3)

        def forward(j):
            for h in (0, 1):
                recv(h, offs[j], 3, "all", 4 + 4 * j)
                send(h, offs[j], 3, "first", 6 + 4 * j, (0, 1))
            for h in (0, 1):
                recv(h, offs[j], 1, "all", 5 + 4 * j)
                send(h, offs[j], 1, "second", 7 + 4 * j, (0, 3))

        def last():
            for j in range(4):
                for h in (0, 1):
                    recv(h, offs[j], 2, "first", 6 + 4 * j)
                    recv(h, offs[j], 2, "second", 7 + 4 * j)

        def drain():
            for cp in started:
                cp.wait_send()

        return [
            start,
            functools.partial(near, 1),
            functools.partial(near, 2),
            functools.partial(forward, 0),
            far,
            functools.partial(forward, 1),
            functools.partial(forward, 2),
            functools.partial(forward, 3),
            last,
            drain,
        ]

    def gather_steps(l):
        lo, hi = pl.ds(0, HALF), pl.ds(HALF, HALF)
        started = []

        def blk(dx, same=True):
            return chip(dx) * 2 + (c if same else 1 - c)

        def send(ref, k, dev):
            cp = rcopy(ref, ref, ags.at[l, k], agr.at[l, k], dev)
            cp.start()
            started.append(cp)

        def recv(ref, k):
            rcopy(ref, ref, ags.at[l, k], agr.at[l, k], partner).wait_recv()

        def start():
            mine = xg.at[blk(0)]
            send(xg.at[blk(0), lo], 1, right)
            send(xg.at[blk(0), hi], 2, left)
            send(xg.at[blk(0), hi], 3, right)
            send(xg.at[blk(0), lo], 4, left)
            send(mine, 0, partner)

        def forward():
            recv(xg.at[blk(3), lo], 1)
            send(xg.at[blk(3), lo], 5, right)
            recv(xg.at[blk(1), hi], 2)
            send(xg.at[blk(1), hi], 6, left)

        def near():
            recv(xg.at[blk(3), hi], 3)
            send(xg.at[blk(3)], 7, partner)
            recv(xg.at[blk(1), lo], 4)
            send(xg.at[blk(1)], 8, partner)

        def far():
            recv(xg.at[blk(2), lo], 5)
            recv(xg.at[blk(2), hi], 6)
            send(xg.at[blk(2)], 9, partner)

        def ready(dx):
            recv(xg.at[blk(dx, False)], {0: 0, 3: 7, 1: 8, 2: 9}[dx])

        def drain():
            for cp in started:
                cp.wait_send()

        return start, forward, near, far, ready, drain

    def normed(values, scale):
        square = jnp.mean(values * values, axis=-1, keepdims=True)
        return (values * lax.rsqrt(square + EPS) * scale[...]).astype(BF16)

    G = 16

    def first_norm():
        def body(i, _):
            r = pl.ds(pl.multiple_of(i * G, G), G)
            xg[tp, r, :] = normed(tok[r, :].astype(F32), s1)
            return 0

        lax.fori_loop(0, ROWS // G, body, 0)

    def ffn_rows(w, first, count):
        lhs = xg[pl.ds(first, count)].reshape(count * ROWS, D)
        dst = pl.ds(first, count)

        def tile(at):
            return w[:, pl.ds(pl.multiple_of(at, 16), 128), :].reshape(D, 128)

        def body(j, _):
            rhs = jnp.concatenate([tile(HID + j * 128), tile(HID + (FULL_TILES + j) * 128)], axis=1)
            r = jnp.dot(lhs, rhs, preferred_element_type=F32)
            g, u = r[:, :128], r[:, 128:]
            h = (g * sigmoid(g) * u).astype(BF16)
            hid[dst, :, pl.ds(pl.multiple_of(j * 128, 128), 128)] = h.reshape(count, ROWS, 128)
            return 0

        lax.fori_loop(0, FULL_TILES, body, 0)
        r = jnp.dot(lhs, tile(HID + 2 * FULL_TILES * 128), preferred_element_type=F32)
        u = pltpu.roll(r, 128 - (HID - FULL_TILES * 128), 1)
        lane = lax.broadcasted_iota(jnp.int32, r.shape, 1)
        h = jnp.where(lane < HID - FULL_TILES * 128, r * sigmoid(r) * u, 0.0).astype(BF16)
        hid[dst, :, pl.ds(FULL_TILES * 128, 128)] = h.reshape(count, ROWS, 128)

    def ffn_in(w, dx):
        ffn_rows(w, 2 * chip(dx), 2)

    def ffn_in_all(w, i):
        ffn_rows(w, 4 * i, 4)

    def mix_in(dx):
        xd = chip(dx)
        lhs = xg[pl.ds(2 * xd, 2)].reshape(2 * ROWS, D)

        def tile(at):
            return w2[:, pl.ds(pl.multiple_of(at, 16), 128), :].reshape(D, 128)

        def body(j, _):
            rhs = jnp.concatenate([tile(CH + j * 128), tile(2 * CH + j * 128)], axis=1)
            r = jnp.dot(lhs, rhs, preferred_element_type=F32).astype(BF16)
            cols = pl.ds(pl.multiple_of(j * 128, 128), 128)
            rc[pl.ds(pl.multiple_of(8 + xd * 256, 8), 256), cols] = r[:, :128].astype(F32)
            br[pl.ds(pl.multiple_of(xd * 256, 256), 256), cols] = r[:, 128:]
            return 0

        lax.fori_loop(0, CH // 128, body, 0)

    def gate_map():
        a = lax.broadcasted_iota(jnp.int32, (BLK, CH), 0)
        b = lax.broadcasted_iota(jnp.int32, (BLK, CH), 1)
        for m, ref in enumerate((decay, inputs)):
            for k in range(2):
                place = jnp.where(b == a + k * BLK, 1.0, 0.0).astype(BF16)
                wide = jnp.dot(ref[k], place, preferred_element_type=F32)
                gb[pl.ds(k * BLK, BLK), pl.ds(m * CH, CH)] = wide.astype(BF16)

    def gates(i):
        at = pl.multiple_of(i * 256, 256)
        tiles = []
        for j in range(CH // 128):
            cols = pl.ds(j * 128, 128)
            window = rc[pl.ds(at, 264), cols]
            acc = window[8:] * ck[3:4, cols]
            for s in (1, 2, 3):
                acc = acc + pltpu.roll(window, s, 0)[8:] * ck[3 - s : 4 - s, cols]
            tiles.append(acc.astype(BF16))
        conv = jnp.concatenate(tiles, axis=1)
        both = jnp.dot(conv, gb[...], preferred_element_type=F32)
        added = jnp.concatenate(
            [jnp.broadcast_to(extra[pl.ds(2 * i + k, 1), :], (128, 128)).T for k in range(2)], axis=0
        )
        weights = -cdw[...]
        rates = -8.0 * (jnp.maximum(weights, 0.0) + jnp.log1p(jnp.exp(-jnp.abs(weights))))
        for j in range(CH // 128):
            cols = pl.ds(j * 128, 128)
            rate = sigmoid(both[:, j * 128 : (j + 1) * 128])
            gate = sigmoid(both[:, CH + j * 128 : CH + (j + 1) * 128])
            log_a = rate * rates[j : j + 1, :] + added
            sa[pl.ds(at, 256), cols] = jnp.exp(log_a)
            sd[pl.ds(at, 256), cols] = (
                jnp.sqrt(one_minus_exp(2.0 * log_a)) * gate * tiles[j].astype(F32)
            )

    T = 64

    def scan_chunk(i, carry):
        r = pl.ds(pl.multiple_of(i * T, T), T)
        a, b = sa[r, :], sd[r, :]
        row = lax.broadcasted_iota(jnp.int32, (T, CH), 0)
        s = 1
        while s < T:
            here = row >= s
            b = a * jnp.where(here, pltpu.roll(b, s, 0), 0.0) + b
            a = a * jnp.where(here, pltpu.roll(a, s, 0), 1.0)
            s *= 2
        state = b + a * carry
        v = br[r, :].astype(F32)
        gelu = 0.5 * v * (1.0 + jnp.tanh(0.7978845608028654 * (v + 0.044715 * v * v * v)))
        hid[i // 2, pl.ds(pl.multiple_of((i % 2) * T, T), T), pl.ds(0, CH)] = (gelu * state).astype(BF16)
        return state[T - 1 : T, :]

    SLOT = {2: 0, 1: 1, 3: 2, 0: 3}

    def project(l, w, depth, dx):
        xd = chip(dx)
        k = SLOT[dx]
        lhs = jnp.concatenate(
            [hid[2 * xd + 1 - c, :, pl.ds(0, depth)], hid[2 * xd + c, :, pl.ds(0, depth)]], axis=0
        )

        def body(n, _):
            rhs = jnp.concatenate([w[4 * n + i, pl.ds(0, depth), :] for i in range(4)], axis=1)
            r = jnp.dot(lhs, rhs, preferred_element_type=F32).astype(BF16)
            cols = pl.ds(pl.multiple_of(n * 512, 512), 512)
            ps[k, :, cols] = r[:ROWS]
            po[k, :, cols] = r[ROWS:]
            return 0

        lax.fori_loop(0, NFS // 4, body, 0)
        rcopy(ps.at[k], pr.at[k], prs.at[l, k], prr.at[l, k], partner).start()

    def pair_ready(l, dx):
        k = SLOT[dx]
        rcopy(ps.at[k], pr.at[k], prs.at[l, k], prr.at[l, k], partner).wait_recv()

    def pair(k, r):
        return po[k, r, :].astype(F32) + pr[k, r, :].astype(F32)

    def ring(l, way, slot):
        return rcopy(
            sb.at[way, slot], rb.at[way, slot], rss.at[l, way, slot], rsr.at[l, way, slot],
            (right, left)[way],
        )

    def post(l, way, slot, dx, base, extra=None):
        def body(i, _):
            at = pl.multiple_of(i * G, G)
            v = pair(SLOT[dx], pl.ds(base + at, G))
            if extra is not None:
                v = v + rb[way, extra, pl.ds(at, G), :].astype(F32)
            sb[way, slot, pl.ds(at, G), :] = v.astype(BF16)
            return 0

        lax.fori_loop(0, HALF // G, body, 0)
        ring(l, way, slot).start()

    def finish(l, before, weight, scale, result):
        ring(l, 0, 2).wait_recv()
        ring(l, 1, 1).wait_recv()
        for base, a, b in ((0, 2, 1), (HALF, 1, 2)):
            if base:
                ring(l, 0, 1).wait_recv()
                ring(l, 1, 2).wait_recv()

            def body(i, _):
                at = pl.multiple_of(i * G, G)
                r = pl.ds(base + at, G)
                v = pair(SLOT[0], r)
                v = v + rb[0, a, pl.ds(at, G), :].astype(F32) + rb[1, b, pl.ds(at, G), :].astype(F32)
                v = (before[r, :].astype(F32) + weight * v).astype(BF16)
                result[r, :] = v
                if scale is not None:
                    xg[tp, r, :] = normed(v.astype(F32), scale)
                return 0

            lax.fori_loop(0, HALF // G, body, 0)

    def reduce(l, w, depth, before, weight, scale, result, steps):
        steps = iter(steps)

        def step():
            for s in next(steps, ()):
                s()

        project(l, w, depth, 2)
        step()
        project(l, w, depth, 1)
        pair_ready(l, 2)
        post(l, 0, 0, 2, 0)
        post(l, 1, 0, 2, HALF)
        step()
        project(l, w, depth, 3)
        pair_ready(l, 1)
        post(l, 0, 1, 1, HALF)
        project(l, w, depth, 0)
        pair_ready(l, 3)
        post(l, 1, 1, 3, 0)
        step()
        ring(l, 0, 0).wait_recv()
        post(l, 0, 2, 1, 0, extra=0)
        ring(l, 1, 0).wait_recv()
        post(l, 1, 2, 3, HALF, extra=0)
        step()
        pair_ready(l, 0)
        finish(l, before, weight, scale, result)
        for k in range(4):
            rcopy(ps.at[k], pr.at[k], prs.at[l, k], prr.at[l, k], partner).wait_send()
        for way in (0, 1):
            for slot in range(3):
                ring(l, way, slot).wait_send()

    barrier = pltpu.get_barrier_semaphore()
    peers = [right, left, partner] + [(fs_of(*d), tp) for d in ((0, 1), (0, 3), (1, 0), (3, 0))]
    for dev in peers:
        pl.semaphore_signal(barrier, inc=1, device_id=dev, device_id_type=MESH)
    load_ffn(w1, g1, u1, d1, wl.at[0])
    load_mix(w2, wl.at[1])
    first_norm()
    pl.semaphore_wait(barrier, len(peers))

    ai = weight_steps(0, w1, IN_CUTS)
    ad = weight_steps(1, w1, DOWN_CUTS)
    a2 = weight_steps(2, w2, MIX_CUTS)
    a3 = weight_steps(3, w3, FFN_CUTS)

    ai[0]()
    start, forward, near, far, ready, drain = gather_steps(0)
    start()
    load_ffn(w3, g3, u3, d3, wl.at[2])
    gate_map()
    rc[pl.ds(0, 8), :] = jnp.zeros((8, CH), F32)
    wait_ffn(w1, d1, wl.at[0])
    wait_load(w2, wl.at[1])
    wait_ffn(w3, d3, wl.at[2])
    ai[1]()
    ai[2]()
    forward()
    ai[3]()
    near()
    ai[4]()
    far()
    ai[5]()
    for dx in (0, 3, 1, 2):
        ready(dx)
    drain()
    ai[6]()
    ai[7]()
    ad[0]()
    ai[8]()
    ad[1]()
    ad[2]()
    ffn_in_all(w1, 0)
    ad[3]()
    ad[4]()
    ffn_in_all(w1, 1)
    for k in (5, 6, 7):
        ad[k]()
    a2[0]()
    ad[8]()
    a2[1]()
    a2[2]()
    reduce(0, w1, HPAD, tok, 0.5, s2, res, [[a2[3]], [a2[4]], [a2[5], a2[6]], [a2[7], a3[0]]])

    start, forward, near, far, ready, drain = gather_steps(1)
    start()
    a2[8]()
    ready(0)
    mix_in(0)
    forward()
    a3[1]()
    near()
    a3[2]()
    ready(3)
    mix_in(3)
    ready(1)
    mix_in(1)
    far()
    a3[3]()
    ready(2)
    mix_in(2)
    drain()
    a3[4]()

    def gate_body(i, _):
        gates(i)
        return 0

    lax.fori_loop(0, SEQ // 256, gate_body, 0)
    a3[5]()
    lax.fori_loop(0, SEQ // T, scan_chunk, jnp.zeros((1, CH), F32))
    reduce(1, w2, CH, res, 1.0, s3, res, [[a3[6]], [], [a3[7]], []])

    start, forward, near, far, ready, drain = gather_steps(2)
    start()
    a3[8]()
    ready(0)
    ffn_in(w3, 0)
    forward()
    near()
    ready(3)
    ffn_in(w3, 3)
    ready(1)
    ffn_in(w3, 1)
    far()
    ready(2)
    ffn_in(w3, 2)
    drain()
    reduce(2, w3, HPAD, res, 0.5, None, out, [])
    ai[9]()
    ad[9]()
    a2[9]()
    a3[9]()


def shards(
    tokens, s1, g1, u1, d1, s2, ri, og, ck, decay, inputs, cdw, extra, mo, s3, g3, u3, d3
):
    vmem = pl.BlockSpec(memory_space=pltpu.VMEM)
    hbm = pl.BlockSpec(memory_space=pl.ANY)
    row = lambda v: v.reshape(1, -1)
    dma = pltpu.SemaphoreType.DMA
    return pl.pallas_call(
        layer_kernel,
        out_shape=jax.ShapeDtypeStruct((ROWS, D), BF16),
        in_specs=[vmem] * 13 + [hbm] * 5,
        out_specs=vmem,
        scratch_shapes=[
            pltpu.VMEM((NFS, FFN_ROWS, 128), BF16),
            pltpu.VMEM((NFS, MIX_ROWS, 128), BF16),
            pltpu.VMEM((NFS, FFN_ROWS, 128), BF16),
            pltpu.VMEM((8, ROWS, D), BF16),
            pltpu.VMEM((8, ROWS, HPAD), BF16),
            pltpu.VMEM((4, ROWS, D), BF16),
            pltpu.VMEM((4, ROWS, D), BF16),
            pltpu.VMEM((4, ROWS, D), BF16),
            pltpu.VMEM((2, 3, HALF, D), BF16),
            pltpu.VMEM((2, 3, HALF, D), BF16),
            pltpu.VMEM((ROWS, D), BF16),
            pltpu.VMEM((SEQ + 8, CH), F32),
            pltpu.VMEM((SEQ, CH), BF16),
            pltpu.VMEM((SEQ, CH), F32),
            pltpu.VMEM((SEQ, CH), F32),
            pltpu.VMEM((CH, 2 * CH), BF16),
            dma((3,)),
            dma((4, 40)),
            dma((4, 40)),
            dma((3, 10)),
            dma((3, 10)),
            dma((3, 4)),
            dma((3, 4)),
            dma((3, 2, 3)),
            dma((3, 2, 3)),
        ],
        compiler_params=pltpu.CompilerParams(
            collective_id=0, has_side_effects=True, vmem_limit_bytes=60 * 1024 * 1024
        ),
        name="layer",
    )(
        tokens, row(s1), row(s2), row(s3),
        g1.T, u1.T, g3.T, u3.T, ck, decay, inputs, cdw.reshape(3, 128), extra.reshape(8, 128),
        d1, ri, og, mo, d3,
    )


def solution(mesh):
    in_specs = (
        P(("fs", "tp"), None), P(), P("fs", "tp"), P("fs", "tp"), P("tp", "fs"),
        P(), P("fs", "tp"), P("fs", "tp"), P(None, "tp"), P("tp", None, None),
        P("tp", None, None), P("tp"), P("fs"), P("tp", "fs"), P(),
        P("fs", "tp"), P("fs", "tp"), P("tp", "fs"),
    )
    out_specs = P(("fs", "tp"), None)
    return jax.shard_map(shards, mesh=mesh, in_specs=in_specs, out_specs=out_specs, check_vma=False)
```

```python
import functools

import jax
import jax.numpy as jnp
from jax import lax
from jax.experimental import pallas as pl
from jax.experimental.pallas import tpu as pltpu
from jax.sharding import PartitionSpec as P

EPS = 1e-06
MESH = pl.DeviceIdType.MESH
F32 = jnp.float32
BF16 = jnp.bfloat16

ROWS = 128
HALF = ROWS // 2
QUART = ROWS // 4
D = 2048
NFS = 16
HID = 688
HPAD = 768
BLK = 192
CH = 384
SEQ = 1024
FULL_TILES = HID // 128
FFN_ROWS = HID + 2 * FULL_TILES * 128 + 128
MIX_ROWS = 3 * CH
FFN_CUTS = (0, 528, 1056, 1584, 2096)
IN_CUTS = (688, 1040, 1392, 1744, 2096)
DOWN_CUTS = (0, 176, 352, 528, 688)
MIX_CUTS = (0, 288, 576, 864, 1152)


def sigmoid(v):
    return 1.0 / (1.0 + jnp.exp(-v))


def one_minus_square(a, v):
    series = 1.0 / 120.0
    for term in (1.0 / 24.0, 1.0 / 6.0, 0.5, 1.0):
        series = term + v * series
    return jnp.where(v > -0.0625, -v * series, 1.0 - a * a)


def layer_kernel(
    tok, s1, s2, s3,
    g1, u1, g3, u3, ck, decay, inputs, cdw, extra,
    d1, ri, og, mo, d3,
    out,
    w1, w2, w3, xg, hid, ps, pr, po, sb, rb, res, rc, br, sa, sd, gb, cv, pde,
    wl, ws, wr, ags, agr, prs, prr, rss, rsr,
):
    fs = lax.axis_index("fs")
    tp = lax.axis_index("tp")
    z, y = fs // 4, fs % 4
    x, c = tp // 2, tp % 2

    def chip(dx):
        return (x + dx) % 4

    def dev_x(dx):
        return (fs, chip(dx) * 2 + c)

    partner = (fs, x * 2 + (1 - c))
    right, left = dev_x(1), dev_x(3)

    def fs_of(dz, dy):
        return ((z + dz) % 4) * 4 + (y + dy) % 4

    def rcopy(src, dst, ssem, rsem, dev):
        return pltpu.make_async_remote_copy(
            src_ref=src, dst_ref=dst, send_sem=ssem, recv_sem=rsem,
            device_id=dev, device_id_type=MESH,
        )

    def load_ffn(w, g, u, d, sem):
        pltpu.make_async_copy(d, w.at[fs, pl.ds(0, HID)], sem).start()
        for j in range(FULL_TILES):
            rows = pl.ds(j * 128, 128)
            w[fs, pl.ds(HID + j * 128, 128), :] = g[rows, :].T
            w[fs, pl.ds(HID + (FULL_TILES + j) * 128, 128), :] = u[rows, :].T
        at = FULL_TILES * 128
        last = jnp.concatenate(
            [g[at:HID, :], u[at:HID, :], jnp.zeros((128 - 2 * (HID - at), 128), BF16)], axis=0
        )
        w[fs, pl.ds(HID + 2 * at, 128), :] = last.T

    def wait_ffn(w, d, sem):
        pltpu.make_async_copy(d, w.at[fs, pl.ds(0, HID)], sem).wait()

    def load_mix(w, sem):
        pltpu.make_async_copy(mo, w.at[fs, pl.ds(0, CH)], sem).start()
        for j in range(CH // 128):
            cols = pl.ds(j * 128, 128)
            pltpu.make_async_copy(ri.at[:, cols], w.at[fs, pl.ds(CH + j * 128, 128)], sem).start()
            pltpu.make_async_copy(og.at[:, cols], w.at[fs, pl.ds(2 * CH + j * 128, 128)], sem).start()

    def wait_load(w, sem):
        pltpu.make_async_copy(w.at[fs], w.at[fs], sem).wait()

    def weight_steps(n, w, cuts):
        def block(h, dp, dq):
            return fs_of(dq, dp) if h == 0 else fs_of(dp, dq)

        def rows(h, part):
            lo, mid, hi = cuts[2 * h], cuts[2 * h + 1], cuts[2 * h + 2]
            a, b = {"all": (lo, hi), "first": (lo, mid), "second": (mid, hi)}[part]
            return pl.ds(a, b - a)

        def desc(h, dp, dq, part, k, to):
            ref = w.at[block(h, dp, dq), rows(h, part)]
            return rcopy(ref, ref, ws.at[n], wr.at[n % 2, 20 * h + k], (block(h, *to), tp))

        def send(*a):
            desc(*a).start()

        def recv(h, dp, dq, part, k):
            desc(h, dp, dq, part, k, (0, 0)).wait_recv()

        offs = (0, 3, 1, 2)

        def start():
            for h in (0, 1):
                send(h, 0, 0, "all", 0, (1, 0))
                send(h, 0, 0, "all", 1, (3, 0))
            for h in (0, 1):
                send(h, 0, 0, "all", 4, (0, 1))
                send(h, 0, 0, "all", 5, (0, 3))

        def across(h, j):
            send(h, offs[j], 0, "all", 4 + 4 * j, (0, 1))
            send(h, offs[j], 0, "all", 5 + 4 * j, (0, 3))

        def near(j):
            for h in (0, 1):
                recv(h, offs[j], 0, "all", j - 1)
                if j == 1:
                    send(h, 3, 0, "first", 2, (1, 0))
                else:
                    send(h, 1, 0, "second", 3, (3, 0))
            for h in (0, 1):
                across(h, j)

        def far():
            for h in (0, 1):
                recv(h, 2, 0, "first", 2)
                recv(h, 2, 0, "second", 3)
                across(h, 3)

        def forward(j):
            for h in (0, 1):
                recv(h, offs[j], 3, "all", 4 + 4 * j)
                send(h, offs[j], 3, "first", 6 + 4 * j, (0, 1))
            for h in (0, 1):
                recv(h, offs[j], 1, "all", 5 + 4 * j)
                send(h, offs[j], 1, "second", 7 + 4 * j, (0, 3))

        def last():
            for j in range(4):
                for h in (0, 1):
                    recv(h, offs[j], 2, "first", 6 + 4 * j)
                    recv(h, offs[j], 2, "second", 7 + 4 * j)

        def drain():
            sent = w.at[pl.ds(0, 15), pl.ds(cuts[0], cuts[4] - cuts[0])]
            pltpu.make_async_copy(sent, sent, ws.at[n]).wait()

        return [
            start,
            functools.partial(near, 1),
            functools.partial(near, 2),
            functools.partial(forward, 0),
            far,
            functools.partial(forward, 1),
            functools.partial(forward, 2),
            functools.partial(forward, 3),
            last,
            drain,
        ]

    def gather_steps(l, m):
        lo, hi, both = pl.ds(HALF * m, QUART), pl.ds(HALF * m + QUART, QUART), pl.ds(HALF * m, HALF)
        def blk(dx, same=True):
            return chip(dx) * 2 + (c if same else 1 - c)

        def send(ref, k, dev):
            rcopy(ref, ref, ags.at[m], agr.at[m, k], dev).start()

        def recv(ref, k):
            rcopy(ref, ref, ags.at[m], agr.at[m, k], partner).wait_recv()

        def start():
            send(xg.at[blk(0), lo], 1, right)
            send(xg.at[blk(0), hi], 2, left)
            send(xg.at[blk(0), hi], 3, right)
            send(xg.at[blk(0), lo], 4, left)
            send(xg.at[blk(0), both], 0, partner)

        def forward():
            recv(xg.at[blk(3), lo], 1)
            send(xg.at[blk(3), lo], 5, right)
            recv(xg.at[blk(1), hi], 2)
            send(xg.at[blk(1), hi], 6, left)

        def near():
            recv(xg.at[blk(3), hi], 3)
            send(xg.at[blk(3), both], 7, partner)
            recv(xg.at[blk(1), lo], 4)
            send(xg.at[blk(1), both], 8, partner)

        def far():
            recv(xg.at[blk(2), lo], 5)
            recv(xg.at[blk(2), hi], 6)
            send(xg.at[blk(2), both], 9, partner)

        def ready():
            for dx, k in ((0, 0), (3, 7), (1, 8), (2, 9)):
                recv(xg.at[blk(dx, False), both], k)
            sent = xg.at[pl.ds(0, 7), both]
            pltpu.make_async_copy(sent, sent, ags.at[m]).wait()

        return start, forward, near, far, ready

    def normed(values, scale):
        square = jnp.mean(values * values, axis=-1, keepdims=True)
        return (values * lax.rsqrt(square + EPS) * scale[...]).astype(BF16)

    G = 16

    def first_norm():
        def body(i, _):
            r = pl.ds(pl.multiple_of(i * G, G), G)
            xg[tp, r, :] = normed(tok[r, :].astype(F32), s1)
            return 0

        lax.fori_loop(0, ROWS // G, body, 0)

    def half_rows(m):
        return xg[:, pl.ds(HALF * m, HALF), :].reshape(8 * HALF, D)

    def ffn_in(w, m, between=()):
        lhs = half_rows(m)
        dst = pl.ds(HALF * m, HALF)

        def tile(at):
            return w[:, pl.ds(pl.multiple_of(at, 16), 128), :].reshape(D, 128)

        def body(j, _):
            rhs = jnp.concatenate([tile(HID + j * 128), tile(HID + (FULL_TILES + j) * 128)], axis=1)
            r = jnp.dot(lhs, rhs, preferred_element_type=F32)
            g, u = r[:, :128], r[:, 128:]
            h = (g * sigmoid(g) * u).astype(BF16)
            hid[:, dst, pl.ds(pl.multiple_of(j * 128, 128), 128)] = h.reshape(8, HALF, 128)
            return 0

        lax.fori_loop(0, 2, body, 0)
        run(between[:1])
        lax.fori_loop(2, 4, body, 0)
        run(between[1:])
        lax.fori_loop(4, FULL_TILES, body, 0)
        r = jnp.dot(lhs, tile(HID + 2 * FULL_TILES * 128), preferred_element_type=F32)
        u = pltpu.roll(r, 128 - (HID - FULL_TILES * 128), 1)
        lane = lax.broadcasted_iota(jnp.int32, r.shape, 1)
        h = jnp.where(lane < HID - FULL_TILES * 128, r * sigmoid(r) * u, 0.0).astype(BF16)
        hid[:, dst, pl.ds(FULL_TILES * 128, 128)] = h.reshape(8, HALF, 128)

    def mix_in(m):
        lhs = half_rows(m)

        def tile(at):
            return w2[:, pl.ds(pl.multiple_of(at, 16), 128), :].reshape(D, 128)

        def body(j, _):
            rhs = jnp.concatenate([tile(CH + j * 128), tile(2 * CH + j * 128)], axis=1)
            r = jnp.dot(lhs, rhs, preferred_element_type=F32).astype(BF16)
            cols = pl.ds(pl.multiple_of(j * 128, 128), 128)
            rc[:, pl.ds(8 + HALF * m, HALF), cols] = r[:, :128].astype(F32).reshape(8, HALF, 128)
            br[:, pl.ds(HALF * m, HALF), cols] = r[:, 128:].reshape(8, HALF, 128)
            return 0

        lax.fori_loop(0, CH // 128, body, 0)

    def gate_map():
        a = lax.broadcasted_iota(jnp.int32, (BLK, CH), 0)
        b = lax.broadcasted_iota(jnp.int32, (BLK, CH), 1)
        for m, ref in enumerate((decay, inputs)):
            for k in range(2):
                place = jnp.where(b == a + k * BLK, 1.0, 0.0).astype(BF16)
                wide = jnp.dot(ref[k], place, preferred_element_type=F32)
                gb[pl.ds(k * BLK, BLK), pl.ds(m * CH, CH)] = wide.astype(BF16)

    def halo():
        rc[0, pl.ds(0, 8), :] = jnp.zeros((8, CH), F32)
        for t in range(1, 8):
            rc[t, pl.ds(0, 8), :] = rc[t - 1, pl.ds(ROWS, 8), :]

    def gate_rates():
        weights = -cdw[...]
        cv[...] = -8.0 * (jnp.maximum(weights, 0.0) + jnp.log1p(jnp.exp(-jnp.abs(weights))))
        for t in range(8):
            pde[t] = jnp.broadcast_to(extra[pl.ds(t, 1), :], (128, 128)).T

    def gates(first, blocks, base, count):
        t = pl.ds(first, blocks)
        size = blocks * count
        dst = pl.ds(base, count)
        tiles = []
        for j in range(CH // 128):
            cols = pl.ds(j * 128, 128)
            rows = []
            for k in range(blocks):
                window = rc[first + k, pl.ds(base, count + 8), cols]
                acc = window[8:] * ck[3:4, cols]
                for s in (1, 2, 3):
                    acc = acc + pltpu.roll(window, s, 0)[8:] * ck[3 - s : 4 - s, cols]
                rows.append(acc)
            tiles.append(jnp.concatenate(rows, axis=0).astype(BF16))
        conv = jnp.concatenate(tiles, axis=1)
        maps = jnp.dot(conv, gb[...], preferred_element_type=F32)
        added = pde[t, dst, :].reshape(size, 128)
        for j in range(CH // 128):
            cols = pl.ds(j * 128, 128)
            rate = sigmoid(maps[:, j * 128 : (j + 1) * 128])
            gate = sigmoid(maps[:, CH + j * 128 : CH + (j + 1) * 128])
            log_a = rate * cv[j : j + 1, :] + added
            a = jnp.exp(log_a)
            drive = jnp.sqrt(one_minus_square(a, 2.0 * log_a)) * gate * tiles[j].astype(F32)
            sa[t, dst, cols] = a.reshape(blocks, count, 128)
            sd[t, dst, cols] = drive.reshape(blocks, count, 128)

    def gates_half(m):
        def body(i, _):
            gates(4 * i, 4, HALF * m, HALF)
            return 0

        lax.fori_loop(0, 2, body, 0)

    T = 64

    def scan_chunk(i, carry):
        r = pl.ds(pl.multiple_of((i % 2) * T, T), T)
        a, b = sa[i // 2, r, :], sd[i // 2, r, :]
        row = lax.broadcasted_iota(jnp.int32, (T, CH), 0)
        s = 1
        while s < T:
            here = row >= s
            b = a * jnp.where(here, pltpu.roll(b, s, 0), 0.0) + b
            a = a * jnp.where(here, pltpu.roll(a, s, 0), 1.0)
            s *= 2
        state = b + a * carry
        v = br[i // 2, r, :].astype(F32)
        gelu = 0.5 * v * (1.0 + jnp.tanh(0.7978845608028654 * (v + 0.044715 * v * v * v)))
        hid[i // 2, r, pl.ds(0, CH)] = (gelu * state).astype(BF16)
        return state[T - 1 : T, :]

    SLOT = {2: 0, 1: 1, 3: 2, 0: 3}

    def pair_copy(l, m, k):
        return rcopy(ps.at[m, k], pr.at[m, k], prs.at[m], prr.at[m, k], partner)

    def project(l, w, depth, m, pair):
        rows = pl.ds(HALF * m, HALF)
        k0 = SLOT[pair[0]]
        lhs = jnp.concatenate(
            [hid[2 * chip(dx) + 1 - c, rows, pl.ds(0, depth)] for dx in pair]
            + [hid[2 * chip(dx) + c, rows, pl.ds(0, depth)] for dx in pair],
            axis=0,
        )

        def body(n, _):
            rhs = jnp.concatenate([w[4 * n + i, pl.ds(0, depth), :] for i in range(4)], axis=1)
            r = jnp.dot(lhs, rhs, preferred_element_type=F32).astype(BF16)
            cols = pl.ds(pl.multiple_of(n * 512, 512), 512)
            ps[m, pl.ds(k0, 2), :, cols] = r[:ROWS].reshape(2, HALF, 512)
            po[m, pl.ds(k0, 2), :, cols] = r[ROWS:].reshape(2, HALF, 512)
            return 0

        lax.fori_loop(0, NFS // 4, body, 0)
        pair_copy(l, m, k0).start()
        pair_copy(l, m, k0 + 1).start()

    def ring(l, m, way, slot):
        return rcopy(
            sb.at[m, way, slot], rb.at[m, way, slot], rss.at[m],
            rsr.at[m, way, slot], (right, left)[way],
        )

    def both(m, k, r):
        return po[m, k, r, :].astype(F32) + pr[m, k, r, :].astype(F32)

    def post(l, m, way, slot, dx, base, extra=None):
        def body(i, _):
            at = pl.multiple_of(i * G, G)
            v = both(m, SLOT[dx], pl.ds(base + at, G))
            if extra is not None:
                v = v + rb[m, way, extra, pl.ds(at, G), :].astype(F32)
            sb[m, way, slot, pl.ds(at, G), :] = v.astype(BF16)
            return 0

        lax.fori_loop(0, QUART // G, body, 0)
        ring(l, m, way, slot).start()

    def post_first(l, m):
        pair_copy(l, m, SLOT[2]).wait_recv()
        post(l, m, 0, 0, 2, 0)
        post(l, m, 1, 0, 2, QUART)
        pair_copy(l, m, SLOT[1]).wait_recv()
        post(l, m, 0, 1, 1, QUART)

    def post_second(l, m):
        pair_copy(l, m, SLOT[3]).wait_recv()
        post(l, m, 1, 1, 3, 0)

    def send_half(l, w, depth, m, between=()):
        project(l, w, depth, m, (2, 1))
        run(between)
        post_first(l, m)
        project(l, w, depth, m, (3, 0))
        post_second(l, m)

    def post_ring(l, m):
        ring(l, m, 0, 0).wait_recv()
        post(l, m, 0, 2, 1, 0, extra=0)
        ring(l, m, 1, 0).wait_recv()
        post(l, m, 1, 2, 3, QUART, extra=0)

    def finish(l, m, before, weight, scale, result):
        pair_copy(l, m, SLOT[0]).wait_recv()
        for way in (0, 1):
            ring(l, m, way, 1).wait_recv()
            ring(l, m, way, 2).wait_recv()
        for base, a, b in ((0, 2, 1), (QUART, 1, 2)):

            def body(i, _):
                at = pl.multiple_of(i * G, G)
                r = pl.ds(HALF * m + base + at, G)
                v = both(m, SLOT[0], pl.ds(base + at, G))
                v = v + rb[m, 0, a, pl.ds(at, G), :].astype(F32) + rb[m, 1, b, pl.ds(at, G), :].astype(F32)
                v = (before[r, :].astype(F32) + weight * v).astype(BF16)
                result[r, :] = v
                if scale is not None:
                    xg[tp, r, :] = normed(v.astype(F32), scale)
                return 0

            lax.fori_loop(0, QUART // G, body, 0)
        pltpu.make_async_copy(ps.at[m], ps.at[m], prs.at[m]).wait()
        pltpu.make_async_copy(sb.at[m], sb.at[m], rss.at[m]).wait()

    def run(steps):
        for s in steps:
            s()

    barrier = pltpu.get_barrier_semaphore()
    peers = [right, left, partner] + [(fs_of(*d), tp) for d in ((0, 1), (0, 3), (1, 0), (3, 0))]
    for dev in peers:
        pl.semaphore_signal(barrier, inc=1, device_id=dev, device_id_type=MESH)
    load_ffn(w1, g1, u1, d1, wl.at[0])
    load_mix(w2, wl.at[1])
    first_norm()
    pl.semaphore_wait(barrier, len(peers))

    ai = weight_steps(0, w1, IN_CUTS)
    ad = weight_steps(1, w1, DOWN_CUTS)
    a2 = weight_steps(2, w2, MIX_CUTS)
    a3 = weight_steps(3, w3, FFN_CUTS)

    ai[0]()
    ga, gc = gather_steps(0, 0), gather_steps(0, 1)
    ga[0]()
    gc[0]()
    load_ffn(w3, g3, u3, d3, wl.at[2])
    gate_map()
    gate_rates()
    rc[:, pl.ds(0, 8), :] = jnp.zeros((8, 8, CH), F32)
    wait_ffn(w1, d1, wl.at[0])
    wait_load(w2, wl.at[1])
    wait_ffn(w3, d3, wl.at[2])
    ai[1]()
    ai[2]()
    ga[1]()
    gc[1]()
    ai[3]()
    ga[2]()
    gc[2]()
    ai[4]()
    ga[3]()
    gc[3]()
    ai[5]()
    ga[4]()
    gc[4]()
    ai[6]()
    ai[7]()
    ad[0]()
    ai[8]()
    ad[1]()
    ad[2]()
    ffn_in(w1, 0, (ad[3], ad[4]))
    ad[5]()
    ffn_in(w1, 1, (ad[6], ad[7]))
    a2[0]()
    ad[8]()

    send_half(0, w1, HPAD, 0)
    run(a2[1:3])
    project(0, w1, HPAD, 1, (2, 1))
    post_ring(0, 0)
    post_first(0, 1)
    project(0, w1, HPAD, 1, (3, 0))
    post_second(0, 1)
    a2[3]()
    ga, gc = gather_steps(1, 0), gather_steps(1, 1)
    finish(0, 0, tok, 0.5, s2, res)
    a2[4]()
    post_ring(0, 1)
    ga[0]()
    run(a2[5:7])
    finish(0, 1, tok, 0.5, s2, res)
    ga[1]()
    gc[0]()
    a2[7]()
    a3[0]()
    ga[2]()
    ga[3]()
    a2[8]()
    ga[4]()
    mix_in(0)
    gc[1]()
    gates_half(0)
    gc[2]()
    gc[3]()
    gc[4]()
    mix_in(1)
    halo()
    gates_half(1)
    gates(0, 8, 0, 8)
    run(a3[1:3])
    lax.fori_loop(0, SEQ // T, scan_chunk, jnp.zeros((1, CH), F32))

    send_half(1, w2, CH, 0)
    a3[3]()
    project(1, w2, CH, 1, (2, 1))
    post_ring(1, 0)
    post_first(1, 1)
    project(1, w2, CH, 1, (3, 0))
    post_second(1, 1)
    a3[4]()
    ga, gc = gather_steps(2, 0), gather_steps(2, 1)
    finish(1, 0, res, 1.0, s3, res)
    post_ring(1, 1)
    ga[0]()
    a3[5]()
    finish(1, 1, res, 1.0, s3, res)
    a3[6]()
    ga[1]()
    gc[0]()
    a3[7]()
    ga[2]()
    ga[3]()
    a3[8]()
    ga[4]()
    ffn_in(w3, 0, (gc[1],))
    send_half(2, w3, HPAD, 0)
    gc[2]()
    gc[3]()
    gc[4]()
    ffn_in(w3, 1, (lambda: post_ring(2, 0),))
    project(2, w3, HPAD, 1, (2, 1))
    post_first(2, 1)
    project(2, w3, HPAD, 1, (3, 0))
    post_second(2, 1)
    finish(2, 0, res, 0.5, None, out)
    ai[9]()
    ad[9]()
    a2[9]()
    a3[9]()
    post_ring(2, 1)
    finish(2, 1, res, 0.5, None, out)


def shards(
    tokens, s1, g1, u1, d1, s2, ri, og, ck, decay, inputs, cdw, extra, mo, s3, g3, u3, d3
):
    vmem = pl.BlockSpec(memory_space=pltpu.VMEM)
    hbm = pl.BlockSpec(memory_space=pl.ANY)
    row = lambda v: v.reshape(1, -1)
    dma = pltpu.SemaphoreType.DMA
    return pl.pallas_call(
        layer_kernel,
        out_shape=jax.ShapeDtypeStruct((ROWS, D), BF16),
        in_specs=[vmem] * 13 + [hbm] * 5,
        out_specs=vmem,
        scratch_shapes=[
            pltpu.VMEM((NFS, FFN_ROWS, 128), BF16),
            pltpu.VMEM((NFS, MIX_ROWS, 128), BF16),
            pltpu.VMEM((NFS, FFN_ROWS, 128), BF16),
            pltpu.VMEM((8, ROWS, D), BF16),
            pltpu.VMEM((8, ROWS, HPAD), BF16),
            pltpu.VMEM((2, 4, HALF, D), BF16),
            pltpu.VMEM((2, 4, HALF, D), BF16),
            pltpu.VMEM((2, 4, HALF, D), BF16),
            pltpu.VMEM((2, 2, 3, QUART, D), BF16),
            pltpu.VMEM((2, 2, 3, QUART, D), BF16),
            pltpu.VMEM((ROWS, D), BF16),
            pltpu.VMEM((8, ROWS + 8, CH), F32),
            pltpu.VMEM((8, ROWS, CH), BF16),
            pltpu.VMEM((8, ROWS, CH), F32),
            pltpu.VMEM((8, ROWS, CH), F32),
            pltpu.VMEM((CH, 2 * CH), BF16),
            pltpu.VMEM((3, 128), F32),
            pltpu.VMEM((8, 128, 128), F32),
            dma((3,)),
            dma((4,)),
            dma((2, 40)),
            dma((2,)),
            dma((2, 10)),
            dma((2,)),
            dma((2, 4)),
            dma((2,)),
            dma((2, 2, 3)),
        ],
        compiler_params=pltpu.CompilerParams(
            collective_id=0, has_side_effects=True, vmem_limit_bytes=60 * 1024 * 1024
        ),
        name="layer",
    )(
        tokens, row(s1), row(s2), row(s3),
        g1.T, u1.T, g3.T, u3.T, ck, decay, inputs, cdw.reshape(3, 128), extra.reshape(8, 128),
        d1, ri, og, mo, d3,
    )


def solution(mesh):
    in_specs = (
        P(("fs", "tp"), None), P(), P("fs", "tp"), P("fs", "tp"), P("tp", "fs"),
        P(), P("fs", "tp"), P("fs", "tp"), P(None, "tp"), P("tp", None, None),
        P("tp", None, None), P("tp"), P("fs"), P("tp", "fs"), P(),
        P("fs", "tp"), P("fs", "tp"), P("tp", "fs"),
    )
    out_specs = P(("fs", "tp"), None)
    return jax.shard_map(shards, mesh=mesh, in_specs=in_specs, out_specs=out_specs, check_vma=False)
```

```python
import functools

import jax
import jax.numpy as jnp
from jax import lax
from jax.experimental import pallas as pl
from jax.experimental.pallas import tpu as pltpu
from jax.sharding import PartitionSpec as P

EPS = 1e-06
MESH = pl.DeviceIdType.MESH
F32 = jnp.float32
BF16 = jnp.bfloat16

ROWS = 128
HALF = ROWS // 2
QUART = ROWS // 4
D = 2048
NFS = 16
HID = 688
HPAD = 768
BLK = 192
CH = 384
SEQ = 1024
FULL_TILES = HID // 128
FFN_ROWS = HID + 2 * FULL_TILES * 128 + 128
MIX_ROWS = 3 * CH
FFN_CUTS = (0, 528, 1056, 1584, 2096)
IN_CUTS = (688, 1040, 1392, 1744, 2096)
DOWN_CUTS = (0, 176, 352, 528, 688)
MIX_CUTS = (0, 288, 576, 864, 1152)


def sigmoid(v):
    return 1.0 / (1.0 + jnp.exp(-v))


def one_minus_square(a, v):
    series = 1.0 / 120.0
    for term in (1.0 / 24.0, 1.0 / 6.0, 0.5, 1.0):
        series = term + v * series
    return jnp.where(v > -0.0625, -v * series, 1.0 - a * a)


def layer_kernel(
    tok_in, s1_in, s2_in, s3_in, g1_in, u1_in, g3_in, u3_in, ck_in, decay_in, inputs_in, cdw_in,
    extra_in, d1, ri, og, mo, d3,
    out_hbm,
    out, tok, s1, s2, s3, g1, u1, g3, u3, ck, decay, inputs, cdw, extra,
    w1, w2, w3, xg, hid, ps, pr, po, sb, rb, res, rc, br, sa, sd, gb, cv, pde,
    fetched, leave, wl, ws, wr, ags, agr, prs, prr, rss, rsr,
):
    fs = lax.axis_index("fs")
    tp = lax.axis_index("tp")
    z, y = fs // 4, fs % 4
    x, c = tp // 2, tp % 2

    def chip(dx):
        return (x + dx) % 4

    def dev_x(dx):
        return (fs, chip(dx) * 2 + c)

    partner = (fs, x * 2 + (1 - c))
    right, left = dev_x(1), dev_x(3)

    def fs_of(dz, dy):
        return ((z + dz) % 4) * 4 + (y + dy) % 4

    def rcopy(src, dst, ssem, rsem, dev):
        return pltpu.make_async_remote_copy(
            src_ref=src, dst_ref=dst, send_sem=ssem, recv_sem=rsem,
            device_id=dev, device_id_type=MESH,
        )

    def load_ffn(w, g, u):
        for j in range(FULL_TILES):
            rows = pl.ds(j * 128, 128)
            w[fs, pl.ds(HID + j * 128, 128), :] = g[rows, :].T
            w[fs, pl.ds(HID + (FULL_TILES + j) * 128, 128), :] = u[rows, :].T
        at = FULL_TILES * 128
        last = jnp.concatenate(
            [g[at:HID, :], u[at:HID, :], jnp.zeros((128 - 2 * (HID - at), 128), BF16)], axis=0
        )
        w[fs, pl.ds(HID + 2 * at, 128), :] = last.T

    def wait_ffn(w, d, sem):
        pltpu.make_async_copy(d, w.at[fs, pl.ds(0, HID)], sem).wait()

    def load_mix(w, sem):
        pltpu.make_async_copy(mo, w.at[fs, pl.ds(0, CH)], sem).start()
        for j in range(CH // 128):
            cols = pl.ds(j * 128, 128)
            pltpu.make_async_copy(ri.at[:, cols], w.at[fs, pl.ds(CH + j * 128, 128)], sem).start()
            pltpu.make_async_copy(og.at[:, cols], w.at[fs, pl.ds(2 * CH + j * 128, 128)], sem).start()

    def wait_load(w, sem):
        pltpu.make_async_copy(w.at[fs], w.at[fs], sem).wait()

    def weight_steps(n, w, cuts):
        def block(h, dp, dq):
            return fs_of(dq, dp) if h == 0 else fs_of(dp, dq)

        def rows(h, part):
            lo, mid, hi = cuts[2 * h], cuts[2 * h + 1], cuts[2 * h + 2]
            a, b = {"all": (lo, hi), "first": (lo, mid), "second": (mid, hi)}[part]
            return pl.ds(a, b - a)

        def desc(h, dp, dq, part, k, to):
            ref = w.at[block(h, dp, dq), rows(h, part)]
            return rcopy(ref, ref, ws.at[n], wr.at[n % 2, 20 * h + k], (block(h, *to), tp))

        def send(*a):
            desc(*a).start()

        def recv(h, dp, dq, part, k):
            desc(h, dp, dq, part, k, (0, 0)).wait_recv()

        offs = (0, 3, 1, 2)

        def start():
            for h in (0, 1):
                send(h, 0, 0, "all", 0, (1, 0))
                send(h, 0, 0, "all", 1, (3, 0))
            for h in (0, 1):
                send(h, 0, 0, "all", 4, (0, 1))
                send(h, 0, 0, "all", 5, (0, 3))

        def across(h, j):
            send(h, offs[j], 0, "all", 4 + 4 * j, (0, 1))
            send(h, offs[j], 0, "all", 5 + 4 * j, (0, 3))

        def near(j):
            for h in (0, 1):
                recv(h, offs[j], 0, "all", j - 1)
                if j == 1:
                    send(h, 3, 0, "first", 2, (1, 0))
                else:
                    send(h, 1, 0, "second", 3, (3, 0))
            for h in (0, 1):
                across(h, j)

        def far():
            for h in (0, 1):
                recv(h, 2, 0, "first", 2)
                recv(h, 2, 0, "second", 3)
                across(h, 3)

        def forward(j):
            for h in (0, 1):
                recv(h, offs[j], 3, "all", 4 + 4 * j)
                send(h, offs[j], 3, "first", 6 + 4 * j, (0, 1))
            for h in (0, 1):
                recv(h, offs[j], 1, "all", 5 + 4 * j)
                send(h, offs[j], 1, "second", 7 + 4 * j, (0, 3))

        def last():
            for j in range(4):
                for h in (0, 1):
                    recv(h, offs[j], 2, "first", 6 + 4 * j)
                    recv(h, offs[j], 2, "second", 7 + 4 * j)

        def drain():
            sent = w.at[pl.ds(0, 15), pl.ds(cuts[0], cuts[4] - cuts[0])]
            pltpu.make_async_copy(sent, sent, ws.at[n]).wait()

        return [
            start,
            functools.partial(near, 1),
            functools.partial(near, 2),
            functools.partial(forward, 0),
            far,
            functools.partial(forward, 1),
            functools.partial(forward, 2),
            functools.partial(forward, 3),
            last,
            drain,
        ]

    def gather_steps(l, m):
        lo, hi, both = pl.ds(HALF * m, QUART), pl.ds(HALF * m + QUART, QUART), pl.ds(HALF * m, HALF)
        def blk(dx, same=True):
            return chip(dx) * 2 + (c if same else 1 - c)

        def send(ref, k, dev):
            rcopy(ref, ref, ags.at[m], agr.at[m, k], dev).start()

        def recv(ref, k):
            rcopy(ref, ref, ags.at[m], agr.at[m, k], partner).wait_recv()

        def start():
            send(xg.at[blk(0), lo], 1, right)
            send(xg.at[blk(0), hi], 2, left)
            send(xg.at[blk(0), hi], 3, right)
            send(xg.at[blk(0), lo], 4, left)
            send(xg.at[blk(0), both], 0, partner)

        def forward():
            recv(xg.at[blk(3), lo], 1)
            send(xg.at[blk(3), lo], 5, right)
            recv(xg.at[blk(1), hi], 2)
            send(xg.at[blk(1), hi], 6, left)

        def near():
            recv(xg.at[blk(3), hi], 3)
            send(xg.at[blk(3), both], 7, partner)
            recv(xg.at[blk(1), lo], 4)
            send(xg.at[blk(1), both], 8, partner)

        def far():
            recv(xg.at[blk(2), lo], 5)
            recv(xg.at[blk(2), hi], 6)
            send(xg.at[blk(2), both], 9, partner)

        def ready():
            for dx, k in ((0, 0), (3, 7), (1, 8), (2, 9)):
                recv(xg.at[blk(dx, False), both], k)
            sent = xg.at[pl.ds(0, 7), both]
            pltpu.make_async_copy(sent, sent, ags.at[m]).wait()

        return start, forward, near, far, ready

    def normed(values, scale):
        square = jnp.mean(values * values, axis=-1, keepdims=True)
        return (values * lax.rsqrt(square + EPS) * scale[...]).astype(BF16)

    G = 16

    def first_norm():
        def body(i, _):
            r = pl.ds(pl.multiple_of(i * G, G), G)
            xg[tp, r, :] = normed(tok[r, :].astype(F32), s1)
            return 0

        lax.fori_loop(0, ROWS // G, body, 0)

    def half_rows(m):
        return xg[:, pl.ds(HALF * m, HALF), :].reshape(8 * HALF, D)

    def ffn_in(w, m, between=()):
        lhs = half_rows(m)
        dst = pl.ds(HALF * m, HALF)

        def tile(at):
            return w[:, pl.ds(pl.multiple_of(at, 16), 128), :].reshape(D, 128)

        def body(j, _):
            rhs = jnp.concatenate([tile(HID + j * 128), tile(HID + (FULL_TILES + j) * 128)], axis=1)
            r = jnp.dot(lhs, rhs, preferred_element_type=F32)
            g, u = r[:, :128], r[:, 128:]
            h = (g * sigmoid(g) * u).astype(BF16)
            hid[:, dst, pl.ds(pl.multiple_of(j * 128, 128), 128)] = h.reshape(8, HALF, 128)
            return 0

        lax.fori_loop(0, 2, body, 0, unroll=True)
        run(between[:1])
        lax.fori_loop(2, 4, body, 0, unroll=True)
        run(between[1:])
        body(4, 0)
        r = jnp.dot(lhs, tile(HID + 2 * FULL_TILES * 128), preferred_element_type=F32)
        u = pltpu.roll(r, 128 - (HID - FULL_TILES * 128), 1)
        lane = lax.broadcasted_iota(jnp.int32, r.shape, 1)
        h = jnp.where(lane < HID - FULL_TILES * 128, r * sigmoid(r) * u, 0.0).astype(BF16)
        hid[:, dst, pl.ds(FULL_TILES * 128, 128)] = h.reshape(8, HALF, 128)

    def mix_in(m):
        lhs = half_rows(m)

        def tile(at):
            return w2[:, pl.ds(pl.multiple_of(at, 16), 128), :].reshape(D, 128)

        def body(j, _):
            rhs = jnp.concatenate([tile(CH + j * 128), tile(2 * CH + j * 128)], axis=1)
            r = jnp.dot(lhs, rhs, preferred_element_type=F32).astype(BF16)
            cols = pl.ds(pl.multiple_of(j * 128, 128), 128)
            rc[:, pl.ds(8 + HALF * m, HALF), cols] = r[:, :128].astype(F32).reshape(8, HALF, 128)
            br[:, pl.ds(HALF * m, HALF), cols] = r[:, 128:].reshape(8, HALF, 128)
            return 0

        lax.fori_loop(0, CH // 128, body, 0, unroll=True)

    def gate_map():
        a = lax.broadcasted_iota(jnp.int32, (BLK, CH), 0)
        b = lax.broadcasted_iota(jnp.int32, (BLK, CH), 1)
        for m, ref in enumerate((decay, inputs)):
            for k in range(2):
                place = jnp.where(b == a + k * BLK, 1.0, 0.0).astype(BF16)
                wide = jnp.dot(ref[k], place, preferred_element_type=F32)
                gb[pl.ds(k * BLK, BLK), pl.ds(m * CH, CH)] = wide.astype(BF16)

    def halo():
        rc[0, pl.ds(0, 8), :] = jnp.zeros((8, CH), F32)
        for t in range(1, 8):
            rc[t, pl.ds(0, 8), :] = rc[t - 1, pl.ds(ROWS, 8), :]

    def gate_rates():
        weights = -cdw[...]
        cv[...] = -8.0 * (jnp.maximum(weights, 0.0) + jnp.log1p(jnp.exp(-jnp.abs(weights))))
        for t in range(8):
            pde[t] = jnp.broadcast_to(extra[pl.ds(t, 1), :], (128, 128)).T

    def gates(first, blocks, base, count):
        t = pl.ds(first, blocks)
        size = blocks * count
        dst = pl.ds(base, count)
        tiles = []
        for j in range(CH // 128):
            cols = pl.ds(j * 128, 128)
            rows = []
            for k in range(blocks):
                window = rc[first + k, pl.ds(base, count + 8), cols]
                acc = window[8:] * ck[3:4, cols]
                for s in (1, 2, 3):
                    acc = acc + pltpu.roll(window, s, 0)[8:] * ck[3 - s : 4 - s, cols]
                rows.append(acc)
            tiles.append(jnp.concatenate(rows, axis=0).astype(BF16))
        conv = jnp.concatenate(tiles, axis=1)
        maps = jnp.dot(conv, gb[...], preferred_element_type=F32)
        added = pde[t, dst, :].reshape(size, 128)
        for j in range(CH // 128):
            cols = pl.ds(j * 128, 128)
            rate = sigmoid(maps[:, j * 128 : (j + 1) * 128])
            gate = sigmoid(maps[:, CH + j * 128 : CH + (j + 1) * 128])
            log_a = rate * cv[j : j + 1, :] + added
            a = jnp.exp(log_a)
            drive = jnp.sqrt(one_minus_square(a, 2.0 * log_a)) * gate * tiles[j].astype(F32)
            sa[t, dst, cols] = a.reshape(blocks, count, 128)
            sd[t, dst, cols] = drive.reshape(blocks, count, 128)

    def gates_half(m):
        def body(i, _):
            gates(4 * i, 4, HALF * m, HALF)
            return 0

        lax.fori_loop(0, 2, body, 0)

    T = 64

    def scan_chunk(i, carry):
        r = pl.ds(pl.multiple_of((i % 2) * T, T), T)
        a, b = sa[i // 2, r, :], sd[i // 2, r, :]
        row = lax.broadcasted_iota(jnp.int32, (T, CH), 0)
        s = 1
        while s < T:
            if s < 8:
                here = row >= s
                b = a * jnp.where(here, pltpu.roll(b, s, 0), 0.0) + b
                a = a * jnp.where(here, pltpu.roll(a, s, 0), 1.0)
            else:
                b = jnp.concatenate([b[:s], a[s:] * b[:-s] + b[s:]], axis=0)
                a = jnp.concatenate([a[:s], a[s:] * a[:-s]], axis=0)
            s *= 2
        state = b + a * carry
        v = br[i // 2, r, :].astype(F32)
        gelu = 0.5 * v * (1.0 + jnp.tanh(0.7978845608028654 * (v + 0.044715 * v * v * v)))
        hid[i // 2, r, pl.ds(0, CH)] = (gelu * state).astype(BF16)
        return state[T - 1 : T, :]

    SLOT = {2: 0, 1: 1, 3: 2, 0: 3}

    def pair_copy(l, m, k):
        return rcopy(ps.at[m, k], pr.at[m, k], prs.at[m], prr.at[m, k], partner)

    def project(l, w, depth, m, pair):
        rows = pl.ds(HALF * m, HALF)
        k0 = SLOT[pair[0]]
        lhs = jnp.concatenate(
            [hid[2 * chip(dx) + 1 - c, rows, pl.ds(0, depth)] for dx in pair]
            + [hid[2 * chip(dx) + c, rows, pl.ds(0, depth)] for dx in pair],
            axis=0,
        )

        def body(n, _):
            rhs = jnp.concatenate([w[4 * n + i, pl.ds(0, depth), :] for i in range(4)], axis=1)
            r = jnp.dot(lhs, rhs, preferred_element_type=F32).astype(BF16)
            cols = pl.ds(pl.multiple_of(n * 512, 512), 512)
            ps[m, pl.ds(k0, 2), :, cols] = r[:ROWS].reshape(2, HALF, 512)
            po[m, pl.ds(k0, 2), :, cols] = r[ROWS:].reshape(2, HALF, 512)
            return 0

        lax.fori_loop(0, NFS // 4, body, 0, unroll=2)
        pair_copy(l, m, k0).start()
        pair_copy(l, m, k0 + 1).start()

    def ring(l, m, way, slot):
        return rcopy(
            sb.at[m, way, slot], rb.at[m, way, slot], rss.at[m],
            rsr.at[m, way, slot], (right, left)[way],
        )

    def both(m, k, r):
        return po[m, k, r, :].astype(F32) + pr[m, k, r, :].astype(F32)

    def post(l, m, way, slot, dx, base, extra=None):
        def body(i, _):
            at = pl.multiple_of(i * G, G)
            v = both(m, SLOT[dx], pl.ds(base + at, G))
            if extra is not None:
                v = v + rb[m, way, extra, pl.ds(at, G), :].astype(F32)
            sb[m, way, slot, pl.ds(at, G), :] = v.astype(BF16)
            return 0

        lax.fori_loop(0, QUART // G, body, 0)
        ring(l, m, way, slot).start()

    def post_first(l, m):
        pair_copy(l, m, SLOT[2]).wait_recv()
        post(l, m, 0, 0, 2, 0)
        post(l, m, 1, 0, 2, QUART)
        pair_copy(l, m, SLOT[1]).wait_recv()
        post(l, m, 0, 1, 1, QUART)

    def post_second(l, m):
        pair_copy(l, m, SLOT[3]).wait_recv()
        post(l, m, 1, 1, 3, 0)

    def send_half(l, w, depth, m, between=()):
        project(l, w, depth, m, (2, 1))
        run(between)
        post_first(l, m)
        project(l, w, depth, m, (3, 0))
        post_second(l, m)

    def post_ring(l, m):
        ring(l, m, 0, 0).wait_recv()
        post(l, m, 0, 2, 1, 0, extra=0)
        ring(l, m, 1, 0).wait_recv()
        post(l, m, 1, 2, 3, QUART, extra=0)

    def finish(l, m, before, weight, scale, result):
        pair_copy(l, m, SLOT[0]).wait_recv()
        for way in (0, 1):
            ring(l, m, way, 1).wait_recv()
            ring(l, m, way, 2).wait_recv()
        for base, a, b in ((0, 2, 1), (QUART, 1, 2)):

            def body(i, _):
                at = pl.multiple_of(i * G, G)
                r = pl.ds(HALF * m + base + at, G)
                v = both(m, SLOT[0], pl.ds(base + at, G))
                v = v + rb[m, 0, a, pl.ds(at, G), :].astype(F32) + rb[m, 1, b, pl.ds(at, G), :].astype(F32)
                v = (before[r, :].astype(F32) + weight * v).astype(BF16)
                result[r, :] = v
                if scale is not None:
                    xg[tp, r, :] = normed(v.astype(F32), scale)
                return 0

            lax.fori_loop(0, QUART // G, body, 0)
        pltpu.make_async_copy(ps.at[m], ps.at[m], prs.at[m]).wait()
        pltpu.make_async_copy(sb.at[m], sb.at[m], rss.at[m]).wait()

    def run(steps):
        for s in steps:
            s()

    barrier = pltpu.get_barrier_semaphore()
    peers = [right, left, partner] + [(fs_of(*d), tp) for d in ((0, 1), (0, 3), (1, 0), (3, 0))]
    for dev in peers:
        pl.semaphore_signal(barrier, inc=1, device_id=dev, device_id_type=MESH)
    def fetch(k, *pairs):
        for src, dst in pairs:
            pltpu.make_async_copy(src, dst, fetched.at[k]).start()

    def fetched_all(k, *refs):
        for ref in refs:
            pltpu.make_async_copy(ref, ref, fetched.at[k]).wait()

    fetch(0, (tok_in, tok))
    fetch(1, (s1_in, s1))
    fetch(2, (g1_in, g1))
    fetch(3, (u1_in, u1))
    later = (
        (s2_in, s2), (s3_in, s3), (g3_in, g3), (u3_in, u3), (ck_in, ck), (decay_in, decay),
        (inputs_in, inputs), (cdw_in, cdw), (extra_in, extra),
    )
    for k, pair in enumerate(later):
        fetch(4 + k, pair)
    pltpu.make_async_copy(d1, w1.at[fs, pl.ds(0, HID)], wl.at[0]).start()
    load_mix(w2, wl.at[1])
    pltpu.make_async_copy(d3, w3.at[fs, pl.ds(0, HID)], wl.at[2]).start()
    fetched_all(2, g1)
    fetched_all(3, u1)
    load_ffn(w1, g1, u1)
    fetched_all(0, tok)
    fetched_all(1, s1)
    first_norm()
    pl.semaphore_wait(barrier, len(peers))

    ai = weight_steps(0, w1, IN_CUTS)
    ad = weight_steps(1, w1, DOWN_CUTS)
    a2 = weight_steps(2, w2, MIX_CUTS)
    a3 = weight_steps(3, w3, FFN_CUTS)

    ai[0]()
    ga, gc = gather_steps(0, 0), gather_steps(0, 1)
    ga[0]()
    gc[0]()
    for k, pair in enumerate(later):
        fetched_all(4 + k, pair[1])
    load_ffn(w3, g3, u3)
    gate_map()
    gate_rates()
    rc[:, pl.ds(0, 8), :] = jnp.zeros((8, 8, CH), F32)
    wait_ffn(w1, d1, wl.at[0])
    wait_load(w2, wl.at[1])
    wait_ffn(w3, d3, wl.at[2])
    ai[1]()
    ai[2]()
    ga[1]()
    gc[1]()
    ai[3]()
    ga[2]()
    gc[2]()
    ai[4]()
    ga[3]()
    gc[3]()
    ai[5]()
    ga[4]()
    gc[4]()
    ai[6]()
    ad[0]()
    ai[7]()
    run(ad[1:4])
    ai[8]()
    ad[4]()
    ffn_in(w1, 0, (ad[5], ad[6]))
    ffn_in(w1, 1, (ad[7],))
    a2[0]()
    ad[8]()

    send_half(0, w1, HPAD, 0)
    run(a2[1:3])
    project(0, w1, HPAD, 1, (2, 1))
    post_ring(0, 0)
    post_first(0, 1)
    project(0, w1, HPAD, 1, (3, 0))
    post_second(0, 1)
    a2[3]()
    ga, gc = gather_steps(1, 0), gather_steps(1, 1)
    finish(0, 0, tok, 0.5, s2, res)
    a2[4]()
    post_ring(0, 1)
    ga[0]()
    run(a2[5:7])
    finish(0, 1, tok, 0.5, s2, res)
    ga[1]()
    gc[0]()
    a2[7]()
    a3[0]()
    ga[2]()
    ga[3]()
    a2[8]()
    ga[4]()
    mix_in(0)
    gc[1]()
    gates_half(0)
    gc[2]()
    gc[3]()
    gc[4]()
    mix_in(1)
    halo()
    gates_half(1)
    gates(0, 8, 0, 8)
    run(a3[1:3])
    lax.fori_loop(0, SEQ // T, scan_chunk, jnp.zeros((1, CH), F32), unroll=2)

    send_half(1, w2, CH, 0)
    a3[3]()
    project(1, w2, CH, 1, (2, 1))
    post_ring(1, 0)
    post_first(1, 1)
    project(1, w2, CH, 1, (3, 0))
    post_second(1, 1)
    a3[4]()
    ga, gc = gather_steps(2, 0), gather_steps(2, 1)
    finish(1, 0, res, 1.0, s3, res)
    post_ring(1, 1)
    ga[0]()
    a3[5]()
    finish(1, 1, res, 1.0, s3, res)
    a3[6]()
    ga[1]()
    gc[0]()
    a3[7]()
    ga[2]()
    ga[3]()
    a3[8]()
    ga[4]()
    ffn_in(w3, 0, (gc[1],))
    gc[2]()
    project(2, w3, HPAD, 0, (2, 1))
    post_first(2, 0)
    gc[3]()
    project(2, w3, HPAD, 0, (3, 0))
    post_second(2, 0)
    gc[4]()
    ffn_in(w3, 1, (lambda: post_ring(2, 0),))
    project(2, w3, HPAD, 1, (2, 1))
    post_first(2, 1)
    project(2, w3, HPAD, 1, (3, 0))
    post_second(2, 1)
    finish(2, 0, res, 0.5, None, out)
    top = pl.ds(0, HALF)
    pltpu.make_async_copy(out.at[top], out_hbm.at[top], leave.at[0]).start()
    ai[9]()
    ad[9]()
    a2[9]()
    a3[9]()
    post_ring(2, 1)
    finish(2, 1, res, 0.5, None, out)
    rest = pl.ds(HALF, HALF)
    pltpu.make_async_copy(out.at[rest], out_hbm.at[rest], leave.at[1]).start()
    for k, r in ((0, top), (1, rest)):
        pltpu.make_async_copy(out.at[r], out_hbm.at[r], leave.at[k]).wait()


def shards(
    tokens, s1, g1, u1, d1, s2, ri, og, ck, decay, inputs, cdw, extra, mo, s3, g3, u3, d3
):
    hbm = pl.BlockSpec(memory_space=pltpu.HBM)
    row = lambda v: v.reshape(1, -1)
    dma = pltpu.SemaphoreType.DMA
    return pl.pallas_call(
        layer_kernel,
        out_shape=jax.ShapeDtypeStruct((ROWS, D), BF16),
        in_specs=[hbm] * 18,
        out_specs=hbm,
        scratch_shapes=[
            pltpu.VMEM((ROWS, D), BF16),
            pltpu.VMEM((ROWS, D), BF16),
            pltpu.VMEM((1, D), F32),
            pltpu.VMEM((1, D), F32),
            pltpu.VMEM((1, D), F32),
            pltpu.VMEM((HID, 128), BF16),
            pltpu.VMEM((HID, 128), BF16),
            pltpu.VMEM((HID, 128), BF16),
            pltpu.VMEM((HID, 128), BF16),
            pltpu.VMEM((4, CH), F32),
            pltpu.VMEM((2, BLK, BLK), BF16),
            pltpu.VMEM((2, BLK, BLK), BF16),
            pltpu.VMEM((3, 128), F32),
            pltpu.VMEM((8, 128), F32),
            pltpu.VMEM((NFS, FFN_ROWS, 128), BF16),
            pltpu.VMEM((NFS, MIX_ROWS, 128), BF16),
            pltpu.VMEM((NFS, FFN_ROWS, 128), BF16),
            pltpu.VMEM((8, ROWS, D), BF16),
            pltpu.VMEM((8, ROWS, HPAD), BF16),
            pltpu.VMEM((2, 4, HALF, D), BF16),
            pltpu.VMEM((2, 4, HALF, D), BF16),
            pltpu.VMEM((2, 4, HALF, D), BF16),
            pltpu.VMEM((2, 2, 3, QUART, D), BF16),
            pltpu.VMEM((2, 2, 3, QUART, D), BF16),
            pltpu.VMEM((ROWS, D), BF16),
            pltpu.VMEM((8, ROWS + 8, CH), F32),
            pltpu.VMEM((8, ROWS, CH), BF16),
            pltpu.VMEM((8, ROWS, CH), F32),
            pltpu.VMEM((8, ROWS, CH), F32),
            pltpu.VMEM((CH, 2 * CH), BF16),
            pltpu.VMEM((3, 128), F32),
            pltpu.VMEM((8, 128, 128), F32),
            dma((13,)),
            dma((2,)),
            dma((3,)),
            dma((4,)),
            dma((2, 40)),
            dma((2,)),
            dma((2, 10)),
            dma((2,)),
            dma((2, 4)),
            dma((2,)),
            dma((2, 2, 3)),
        ],
        compiler_params=pltpu.CompilerParams(
            collective_id=0, has_side_effects=True, vmem_limit_bytes=62 * 1024 * 1024
        ),
        name="layer",
    )(
        tokens, row(s1), row(s2), row(s3),
        g1.T, u1.T, g3.T, u3.T, ck, decay, inputs, cdw.reshape(3, 128), extra.reshape(8, 128),
        d1, ri, og, mo, d3,
    )


def solution(mesh):
    in_specs = (
        P(("fs", "tp"), None), P(), P("fs", "tp"), P("fs", "tp"), P("tp", "fs"),
        P(), P("fs", "tp"), P("fs", "tp"), P(None, "tp"), P("tp", None, None),
        P("tp", None, None), P("tp"), P("fs"), P("tp", "fs"), P(),
        P("fs", "tp"), P("fs", "tp"), P("tp", "fs"),
    )
    out_specs = P(("fs", "tp"), None)
    return jax.shard_map(shards, mesh=mesh, in_specs=in_specs, out_specs=out_specs, check_vma=False)
```

```python
import functools

import jax
import jax.numpy as jnp
from jax import lax
from jax.experimental import pallas as pl
from jax.experimental.pallas import tpu as pltpu
from jax.sharding import PartitionSpec as P

EPS = 1e-06
MESH = pl.DeviceIdType.MESH
F32 = jnp.float32
BF16 = jnp.bfloat16

ROWS = 128
HALF = ROWS // 2
QUART = ROWS // 4
D = 2048
NFS = 16
HID = 688
HPAD = 768
BLK = 192
CH = 384
SEQ = 1024
FULL_TILES = HID // 128
FFN_ROWS = HID + 2 * FULL_TILES * 128 + 128
MIX_ROWS = 3 * CH
FFN_CUTS = (0, 528, 1056, 1584, 2096)
IN_CUTS = (688, 1040, 1392, 1744, 2096)
DOWN_CUTS = (0, 176, 352, 528, 688)
MIX_CUTS = (0, 288, 576, 864, 1152)


def sigmoid(v):
    return 1.0 / (1.0 + jnp.exp(-v))


def one_minus_square(a, v):
    series = 1.0 / 120.0
    for term in (1.0 / 24.0, 1.0 / 6.0, 0.5, 1.0):
        series = term + v * series
    return jnp.where(v > -0.0625, -v * series, 1.0 - a * a)


def layer_kernel(
    tok_in, s1_in, s2_in, s3_in, g1_in, u1_in, g3_in, u3_in, ck_in, decay_in, inputs_in, cdw_in,
    extra_in, d1, ri, og, mo, d3,
    out_hbm,
    out, tok, s1, s2, s3, g1, u1, g3, u3, ck, decay, inputs, cdw, extra,
    w1, w2, w3, xg, hid, ps, pr, po, sb, rb, res, rc, br, sa, sd, gb, cv, pde,
    fetched, leave, wl, ws, wr, ags, agr, prs, prr, rss, rsr,
):
    fs = lax.axis_index("fs")
    tp = lax.axis_index("tp")
    z, y = fs // 4, fs % 4
    x, c = tp // 2, tp % 2

    def chip(dx):
        return (x + dx) % 4

    def dev_x(dx):
        return (fs, chip(dx) * 2 + c)

    partner = (fs, x * 2 + (1 - c))
    right, left = dev_x(1), dev_x(3)

    def fs_of(dz, dy):
        return ((z + dz) % 4) * 4 + (y + dy) % 4

    def rcopy(src, dst, ssem, rsem, dev):
        return pltpu.make_async_remote_copy(
            src_ref=src, dst_ref=dst, send_sem=ssem, recv_sem=rsem,
            device_id=dev, device_id_type=MESH,
        )

    def load_ffn(w, g, u):
        for j in range(FULL_TILES):
            rows = pl.ds(j * 128, 128)
            w[fs, pl.ds(HID + j * 128, 128), :] = g[rows, :].T
            w[fs, pl.ds(HID + (FULL_TILES + j) * 128, 128), :] = u[rows, :].T
        at = FULL_TILES * 128
        last = jnp.concatenate(
            [g[at:HID, :], u[at:HID, :], jnp.zeros((128 - 2 * (HID - at), 128), BF16)], axis=0
        )
        w[fs, pl.ds(HID + 2 * at, 128), :] = last.T

    def wait_ffn(w, d, sem):
        pltpu.make_async_copy(d, w.at[fs, pl.ds(0, HID)], sem).wait()

    def load_mix(w, sem):
        pltpu.make_async_copy(mo, w.at[fs, pl.ds(0, CH)], sem).start()
        for j in range(CH // 128):
            cols = pl.ds(j * 128, 128)
            pltpu.make_async_copy(ri.at[:, cols], w.at[fs, pl.ds(CH + j * 128, 128)], sem).start()
            pltpu.make_async_copy(og.at[:, cols], w.at[fs, pl.ds(2 * CH + j * 128, 128)], sem).start()

    def wait_load(w, sem):
        pltpu.make_async_copy(w.at[fs], w.at[fs], sem).wait()

    def weight_steps(n, w, cuts):
        def block(h, dp, dq):
            return fs_of(dq, dp) if h == 0 else fs_of(dp, dq)

        def rows(h, part):
            lo, mid, hi = cuts[2 * h], cuts[2 * h + 1], cuts[2 * h + 2]
            a, b = {"all": (lo, hi), "first": (lo, mid), "second": (mid, hi)}[part]
            return pl.ds(a, b - a)

        def desc(h, dp, dq, part, k, to):
            ref = w.at[block(h, dp, dq), rows(h, part)]
            return rcopy(ref, ref, ws.at[n], wr.at[n % 2, 20 * h + k], (block(h, *to), tp))

        def send(*a):
            desc(*a).start()

        def recv(h, dp, dq, part, k):
            desc(h, dp, dq, part, k, (0, 0)).wait_recv()

        offs = (0, 3, 1, 2)

        def start():
            for h in (0, 1):
                send(h, 0, 0, "all", 0, (1, 0))
                send(h, 0, 0, "all", 1, (3, 0))
            for h in (0, 1):
                send(h, 0, 0, "all", 4, (0, 1))
                send(h, 0, 0, "all", 5, (0, 3))

        def across(h, j):
            send(h, offs[j], 0, "all", 4 + 4 * j, (0, 1))
            send(h, offs[j], 0, "all", 5 + 4 * j, (0, 3))

        def near(j):
            for h in (0, 1):
                recv(h, offs[j], 0, "all", j - 1)
                if j == 1:
                    send(h, 3, 0, "first", 2, (1, 0))
                else:
                    send(h, 1, 0, "second", 3, (3, 0))
            for h in (0, 1):
                across(h, j)

        def far():
            for h in (0, 1):
                recv(h, 2, 0, "first", 2)
                recv(h, 2, 0, "second", 3)
                across(h, 3)

        def forward(j):
            for h in (0, 1):
                recv(h, offs[j], 3, "all", 4 + 4 * j)
                send(h, offs[j], 3, "first", 6 + 4 * j, (0, 1))
            for h in (0, 1):
                recv(h, offs[j], 1, "all", 5 + 4 * j)
                send(h, offs[j], 1, "second", 7 + 4 * j, (0, 3))

        def last():
            for j in range(4):
                for h in (0, 1):
                    recv(h, offs[j], 2, "first", 6 + 4 * j)
                    recv(h, offs[j], 2, "second", 7 + 4 * j)

        def drain():
            sent = w.at[pl.ds(0, 15), pl.ds(cuts[0], cuts[4] - cuts[0])]
            pltpu.make_async_copy(sent, sent, ws.at[n]).wait()

        return [
            start,
            functools.partial(near, 1),
            functools.partial(near, 2),
            functools.partial(forward, 0),
            far,
            functools.partial(forward, 1),
            functools.partial(forward, 2),
            functools.partial(forward, 3),
            last,
            drain,
        ]

    def gather_steps(l, m):
        lo, hi, both = pl.ds(HALF * m, QUART), pl.ds(HALF * m + QUART, QUART), pl.ds(HALF * m, HALF)
        def blk(dx, same=True):
            return chip(dx) * 2 + (c if same else 1 - c)

        def send(ref, k, dev):
            rcopy(ref, ref, ags.at[m], agr.at[m, k], dev).start()

        def recv(ref, k):
            rcopy(ref, ref, ags.at[m], agr.at[m, k], partner).wait_recv()

        def start():
            send(xg.at[blk(0), lo], 1, right)
            send(xg.at[blk(0), hi], 2, left)
            send(xg.at[blk(0), hi], 3, right)
            send(xg.at[blk(0), lo], 4, left)
            send(xg.at[blk(0), both], 0, partner)

        def forward():
            recv(xg.at[blk(3), lo], 1)
            send(xg.at[blk(3), lo], 5, right)
            recv(xg.at[blk(1), hi], 2)
            send(xg.at[blk(1), hi], 6, left)

        def near():
            recv(xg.at[blk(3), hi], 3)
            send(xg.at[blk(3), both], 7, partner)
            recv(xg.at[blk(1), lo], 4)
            send(xg.at[blk(1), both], 8, partner)

        def far():
            recv(xg.at[blk(2), lo], 5)
            recv(xg.at[blk(2), hi], 6)
            send(xg.at[blk(2), both], 9, partner)

        def ready():
            for dx, k in ((0, 0), (3, 7), (1, 8), (2, 9)):
                recv(xg.at[blk(dx, False), both], k)
            sent = xg.at[pl.ds(0, 7), both]
            pltpu.make_async_copy(sent, sent, ags.at[m]).wait()

        return start, forward, near, far, ready

    def normed(values, scale):
        square = jnp.mean(values * values, axis=-1, keepdims=True)
        return (values * lax.rsqrt(square + EPS) * scale[...]).astype(BF16)

    G = 16

    def first_norm():
        def body(i, _):
            r = pl.ds(pl.multiple_of(i * G, G), G)
            xg[tp, r, :] = normed(tok[r, :].astype(F32), s1)
            return 0

        lax.fori_loop(0, ROWS // G, body, 0)

    def half_rows(m):
        return xg[:, pl.ds(HALF * m, HALF), :].reshape(8 * HALF, D)

    def ffn_in(w, m, between=()):
        lhs = half_rows(m)
        dst = pl.ds(HALF * m, HALF)

        def tile(at):
            return w[:, pl.ds(pl.multiple_of(at, 16), 128), :].reshape(D, 128)

        def body(j, _):
            rhs = jnp.concatenate([tile(HID + j * 128), tile(HID + (FULL_TILES + j) * 128)], axis=1)
            r = jnp.dot(lhs, rhs, preferred_element_type=F32)
            g, u = r[:, :128], r[:, 128:]
            h = (g * sigmoid(g) * u).astype(BF16)
            hid[:, dst, pl.ds(pl.multiple_of(j * 128, 128), 128)] = h.reshape(8, HALF, 128)
            return 0

        lax.fori_loop(0, 2, body, 0, unroll=True)
        run(between[:1])
        lax.fori_loop(2, 4, body, 0, unroll=True)
        run(between[1:])
        body(4, 0)
        r = jnp.dot(lhs, tile(HID + 2 * FULL_TILES * 128), preferred_element_type=F32)
        u = pltpu.roll(r, 128 - (HID - FULL_TILES * 128), 1)
        lane = lax.broadcasted_iota(jnp.int32, r.shape, 1)
        h = jnp.where(lane < HID - FULL_TILES * 128, r * sigmoid(r) * u, 0.0).astype(BF16)
        hid[:, dst, pl.ds(FULL_TILES * 128, 128)] = h.reshape(8, HALF, 128)

    def mix_in(m):
        lhs = half_rows(m)

        def tile(at):
            return w2[:, pl.ds(pl.multiple_of(at, 16), 128), :].reshape(D, 128)

        def body(j, _):
            rhs = jnp.concatenate([tile(CH + j * 128), tile(2 * CH + j * 128)], axis=1)
            r = jnp.dot(lhs, rhs, preferred_element_type=F32).astype(BF16)
            cols = pl.ds(pl.multiple_of(j * 128, 128), 128)
            rc[:, pl.ds(8 + HALF * m, HALF), cols] = r[:, :128].astype(F32).reshape(8, HALF, 128)
            v = r[:, 128:].astype(F32)
            v = 0.5 * v * (1.0 + jnp.tanh(0.7978845608028654 * (v + 0.044715 * v * v * v)))
            br[:, pl.ds(HALF * m, HALF), cols] = v.reshape(8, HALF, 128)
            return 0

        lax.fori_loop(0, CH // 128, body, 0, unroll=True)

    def gate_map():
        a = lax.broadcasted_iota(jnp.int32, (BLK, CH), 0)
        b = lax.broadcasted_iota(jnp.int32, (BLK, CH), 1)
        for m, ref in enumerate((decay, inputs)):
            for k in range(2):
                place = jnp.where(b == a + k * BLK, 1.0, 0.0).astype(BF16)
                wide = jnp.dot(ref[k], place, preferred_element_type=F32)
                gb[pl.ds(k * BLK, BLK), pl.ds(m * CH, CH)] = wide.astype(BF16)

    def halo():
        rc[0, pl.ds(0, 8), :] = jnp.zeros((8, CH), F32)
        for t in range(1, 8):
            rc[t, pl.ds(0, 8), :] = rc[t - 1, pl.ds(ROWS, 8), :]

    def gate_rates():
        weights = -cdw[...]
        cv[...] = -8.0 * (jnp.maximum(weights, 0.0) + jnp.log1p(jnp.exp(-jnp.abs(weights))))
        for t in range(8):
            pde[t] = jnp.broadcast_to(extra[pl.ds(t, 1), :], (128, 128)).T

    def gates(first, blocks, base, count):
        t = pl.ds(first, blocks)
        size = blocks * count
        dst = pl.ds(base, count)
        tiles = []
        for j in range(CH // 128):
            cols = pl.ds(j * 128, 128)
            rows = []
            for k in range(blocks):
                window = rc[first + k, pl.ds(base, count + 8), cols]
                acc = window[8:] * ck[3:4, cols]
                for s in (1, 2, 3):
                    acc = acc + pltpu.roll(window, s, 0)[8:] * ck[3 - s : 4 - s, cols]
                rows.append(acc)
            tiles.append(jnp.concatenate(rows, axis=0).astype(BF16))
        conv = jnp.concatenate(tiles, axis=1)
        maps = jnp.dot(conv, gb[...], preferred_element_type=F32)
        added = pde[t, dst, :].reshape(size, 128)
        for j in range(CH // 128):
            cols = pl.ds(j * 128, 128)
            rate = sigmoid(maps[:, j * 128 : (j + 1) * 128])
            gate = sigmoid(maps[:, CH + j * 128 : CH + (j + 1) * 128])
            log_a = rate * cv[j : j + 1, :] + added
            a = jnp.exp(log_a)
            drive = jnp.sqrt(one_minus_square(a, 2.0 * log_a)) * gate * tiles[j].astype(F32)
            sa[t, dst, cols] = a.reshape(blocks, count, 128)
            sd[t, dst, cols] = drive.reshape(blocks, count, 128)

    def gates_half(m):
        def body(i, _):
            gates(4 * i, 4, HALF * m, HALF)
            return 0

        lax.fori_loop(0, 2, body, 0, unroll=True)

    T = 64

    def scan_chunk(i, carry):
        r = pl.ds(pl.multiple_of((i % 2) * T, T), T)
        a, b = sa[i // 2, r, :], sd[i // 2, r, :]
        row = lax.broadcasted_iota(jnp.int32, (T, CH), 0)
        s = 1
        while s < T:
            if s < 8:
                here = row >= s
                b = a * jnp.where(here, pltpu.roll(b, s, 0), 0.0) + b
                a = a * jnp.where(here, pltpu.roll(a, s, 0), 1.0)
            else:
                b = jnp.concatenate([b[:s], a[s:] * b[:-s] + b[s:]], axis=0)
                a = jnp.concatenate([a[:s], a[s:] * a[:-s]], axis=0)
            s *= 2
        state = b + a * carry
        hid[i // 2, r, pl.ds(0, CH)] = (br[i // 2, r, :] * state).astype(BF16)
        return state[T - 1 : T, :]

    SLOT = {2: 0, 1: 1, 3: 2, 0: 3}

    def pair_copy(l, m, k):
        return rcopy(ps.at[m, k], pr.at[m, k], prs.at[m], prr.at[m, k], partner)

    def project(l, w, depth, m, pair):
        rows = pl.ds(HALF * m, HALF)
        k0 = SLOT[pair[0]]
        lhs = jnp.concatenate(
            [hid[2 * chip(dx) + 1 - c, rows, pl.ds(0, depth)] for dx in pair]
            + [hid[2 * chip(dx) + c, rows, pl.ds(0, depth)] for dx in pair],
            axis=0,
        )

        def body(n, _):
            rhs = jnp.concatenate([w[4 * n + i, pl.ds(0, depth), :] for i in range(4)], axis=1)
            r = jnp.dot(lhs, rhs, preferred_element_type=F32).astype(BF16)
            cols = pl.ds(pl.multiple_of(n * 512, 512), 512)
            ps[m, pl.ds(k0, 2), :, cols] = r[:ROWS].reshape(2, HALF, 512)
            po[m, pl.ds(k0, 2), :, cols] = r[ROWS:].reshape(2, HALF, 512)
            return 0

        lax.fori_loop(0, NFS // 4, body, 0, unroll=True)
        pair_copy(l, m, k0).start()
        pair_copy(l, m, k0 + 1).start()

    def ring(l, m, way, slot):
        return rcopy(
            sb.at[m, way, slot], rb.at[m, way, slot], rss.at[m],
            rsr.at[m, way, slot], (right, left)[way],
        )

    def both(m, k, r):
        return po[m, k, r, :].astype(F32) + pr[m, k, r, :].astype(F32)

    def post(l, m, way, slot, dx, base, extra=None):
        def body(i, _):
            at = pl.multiple_of(i * G, G)
            v = both(m, SLOT[dx], pl.ds(base + at, G))
            if extra is not None:
                v = v + rb[m, way, extra, pl.ds(at, G), :].astype(F32)
            sb[m, way, slot, pl.ds(at, G), :] = v.astype(BF16)
            return 0

        lax.fori_loop(0, QUART // G, body, 0)
        ring(l, m, way, slot).start()

    def post_first(l, m):
        pair_copy(l, m, SLOT[2]).wait_recv()
        post(l, m, 0, 0, 2, 0)
        post(l, m, 1, 0, 2, QUART)
        pair_copy(l, m, SLOT[1]).wait_recv()
        post(l, m, 0, 1, 1, QUART)

    def post_second(l, m):
        pair_copy(l, m, SLOT[3]).wait_recv()
        post(l, m, 1, 1, 3, 0)

    def send_half(l, w, depth, m, between=()):
        project(l, w, depth, m, (2, 1))
        run(between)
        post_first(l, m)
        project(l, w, depth, m, (3, 0))
        post_second(l, m)

    def post_ring(l, m):
        ring(l, m, 0, 0).wait_recv()
        post(l, m, 0, 2, 1, 0, extra=0)
        ring(l, m, 1, 0).wait_recv()
        post(l, m, 1, 2, 3, QUART, extra=0)

    def finish(l, m, before, weight, scale, result):
        pair_copy(l, m, SLOT[0]).wait_recv()
        for way in (0, 1):
            ring(l, m, way, 1).wait_recv()
            ring(l, m, way, 2).wait_recv()
        for base, a, b in ((0, 2, 1), (QUART, 1, 2)):

            def body(i, _):
                at = pl.multiple_of(i * G, G)
                r = pl.ds(HALF * m + base + at, G)
                v = both(m, SLOT[0], pl.ds(base + at, G))
                v = v + rb[m, 0, a, pl.ds(at, G), :].astype(F32) + rb[m, 1, b, pl.ds(at, G), :].astype(F32)
                v = (before[r, :].astype(F32) + weight * v).astype(BF16)
                result[r, :] = v
                if scale is not None:
                    xg[tp, r, :] = normed(v.astype(F32), scale)
                return 0

            lax.fori_loop(0, QUART // G, body, 0)
        pltpu.make_async_copy(ps.at[m], ps.at[m], prs.at[m]).wait()
        pltpu.make_async_copy(sb.at[m], sb.at[m], rss.at[m]).wait()

    def run(steps):
        for s in steps:
            s()

    barrier = pltpu.get_barrier_semaphore()
    peers = [right, left, partner] + [(fs_of(*d), tp) for d in ((0, 1), (0, 3), (1, 0), (3, 0))]
    for dev in peers:
        pl.semaphore_signal(barrier, inc=1, device_id=dev, device_id_type=MESH)
    def fetch(k, *pairs):
        for src, dst in pairs:
            pltpu.make_async_copy(src, dst, fetched.at[k]).start()

    def fetched_all(k, *refs):
        for ref in refs:
            pltpu.make_async_copy(ref, ref, fetched.at[k]).wait()

    fetch(0, (tok_in, tok))
    fetch(1, (s1_in, s1))
    fetch(2, (g1_in, g1))
    fetch(3, (u1_in, u1))
    later = (
        (s2_in, s2), (s3_in, s3), (g3_in, g3), (u3_in, u3), (ck_in, ck), (decay_in, decay),
        (inputs_in, inputs), (cdw_in, cdw), (extra_in, extra),
    )
    for k, pair in enumerate(later):
        fetch(4 + k, pair)
    pltpu.make_async_copy(d1, w1.at[fs, pl.ds(0, HID)], wl.at[0]).start()
    load_mix(w2, wl.at[1])
    pltpu.make_async_copy(d3, w3.at[fs, pl.ds(0, HID)], wl.at[2]).start()
    fetched_all(2, g1)
    fetched_all(3, u1)
    load_ffn(w1, g1, u1)
    fetched_all(0, tok)
    fetched_all(1, s1)
    first_norm()
    pl.semaphore_wait(barrier, len(peers))

    ai = weight_steps(0, w1, IN_CUTS)
    ad = weight_steps(1, w1, DOWN_CUTS)
    a2 = weight_steps(2, w2, MIX_CUTS)
    a3 = weight_steps(3, w3, FFN_CUTS)

    ai[0]()
    ga, gc = gather_steps(0, 0), gather_steps(0, 1)
    ga[0]()
    gc[0]()
    for k, pair in enumerate(later):
        fetched_all(4 + k, pair[1])
    load_ffn(w3, g3, u3)
    gate_map()
    gate_rates()
    rc[:, pl.ds(0, 8), :] = jnp.zeros((8, 8, CH), F32)
    wait_ffn(w1, d1, wl.at[0])
    wait_load(w2, wl.at[1])
    wait_ffn(w3, d3, wl.at[2])
    ai[1]()
    ai[2]()
    ga[1]()
    gc[1]()
    ai[3]()
    ga[2]()
    gc[2]()
    ai[4]()
    ga[3]()
    gc[3]()
    ai[5]()
    ga[4]()
    gc[4]()
    ai[6]()
    ad[0]()
    ai[7]()
    run(ad[1:4])
    ai[8]()
    ad[4]()
    ffn_in(w1, 0, (ad[5], ad[6]))
    ffn_in(w1, 1, (ad[7],))
    a2[0]()
    ad[8]()

    send_half(0, w1, HPAD, 0)
    run(a2[1:3])
    project(0, w1, HPAD, 1, (2, 1))
    post_ring(0, 0)
    post_first(0, 1)
    project(0, w1, HPAD, 1, (3, 0))
    post_second(0, 1)
    a2[3]()
    ga, gc = gather_steps(1, 0), gather_steps(1, 1)
    finish(0, 0, tok, 0.5, s2, res)
    a2[4]()
    post_ring(0, 1)
    ga[0]()
    run(a2[5:7])
    finish(0, 1, tok, 0.5, s2, res)
    ga[1]()
    gc[0]()
    a2[7]()
    a3[0]()
    ga[2]()
    ga[3]()
    a2[8]()
    ga[4]()
    mix_in(0)
    gc[1]()
    gates_half(0)
    gc[2]()
    gc[3]()
    gc[4]()
    mix_in(1)
    halo()
    gates_half(1)
    gates(0, 8, 0, 8)
    run(a3[1:3])
    lax.fori_loop(0, SEQ // T, scan_chunk, jnp.zeros((1, CH), F32), unroll=4)

    send_half(1, w2, CH, 0)
    a3[3]()
    project(1, w2, CH, 1, (2, 1))
    post_ring(1, 0)
    post_first(1, 1)
    project(1, w2, CH, 1, (3, 0))
    post_second(1, 1)
    a3[4]()
    ga, gc = gather_steps(2, 0), gather_steps(2, 1)
    finish(1, 0, res, 1.0, s3, res)
    post_ring(1, 1)
    ga[0]()
    a3[5]()
    finish(1, 1, res, 1.0, s3, res)
    a3[6]()
    ga[1]()
    gc[0]()
    a3[7]()
    ga[2]()
    ga[3]()
    a3[8]()
    ga[4]()
    ffn_in(w3, 0, (gc[1],))
    gc[2]()
    project(2, w3, HPAD, 0, (2, 1))
    project(2, w3, HPAD, 0, (3, 0))
    post_first(2, 0)
    gc[3]()
    post_second(2, 0)
    gc[4]()
    ffn_in(w3, 1, (lambda: None, lambda: post_ring(2, 0)))
    project(2, w3, HPAD, 1, (2, 1))
    project(2, w3, HPAD, 1, (3, 0))
    post_first(2, 1)
    post_second(2, 1)
    finish(2, 0, res, 0.5, None, out)
    top = pl.ds(0, HALF)
    pltpu.make_async_copy(out.at[top], out_hbm.at[top], leave.at[0]).start()
    ai[9]()
    ad[9]()
    a2[9]()
    a3[9]()
    post_ring(2, 1)
    finish(2, 1, res, 0.5, None, out)
    rest = pl.ds(HALF, HALF)
    pltpu.make_async_copy(out.at[rest], out_hbm.at[rest], leave.at[1]).start()
    for k, r in ((0, top), (1, rest)):
        pltpu.make_async_copy(out.at[r], out_hbm.at[r], leave.at[k]).wait()


def shards(
    tokens, s1, g1, u1, d1, s2, ri, og, ck, decay, inputs, cdw, extra, mo, s3, g3, u3, d3
):
    hbm = pl.BlockSpec(memory_space=pltpu.HBM)
    row = lambda v: v.reshape(1, -1)
    dma = pltpu.SemaphoreType.DMA
    return pl.pallas_call(
        layer_kernel,
        out_shape=jax.ShapeDtypeStruct((ROWS, D), BF16),
        in_specs=[hbm] * 18,
        out_specs=hbm,
        scratch_shapes=[
            pltpu.VMEM((ROWS, D), BF16),
            pltpu.VMEM((ROWS, D), BF16),
            pltpu.VMEM((1, D), F32),
            pltpu.VMEM((1, D), F32),
            pltpu.VMEM((1, D), F32),
            pltpu.VMEM((HID, 128), BF16),
            pltpu.VMEM((HID, 128), BF16),
            pltpu.VMEM((HID, 128), BF16),
            pltpu.VMEM((HID, 128), BF16),
            pltpu.VMEM((4, CH), F32),
            pltpu.VMEM((2, BLK, BLK), BF16),
            pltpu.VMEM((2, BLK, BLK), BF16),
            pltpu.VMEM((3, 128), F32),
            pltpu.VMEM((8, 128), F32),
            pltpu.VMEM((NFS, FFN_ROWS, 128), BF16),
            pltpu.VMEM((NFS, MIX_ROWS, 128), BF16),
            pltpu.VMEM((NFS, FFN_ROWS, 128), BF16),
            pltpu.VMEM((8, ROWS, D), BF16),
            pltpu.VMEM((8, ROWS, HPAD), BF16),
            pltpu.VMEM((2, 4, HALF, D), BF16),
            pltpu.VMEM((2, 4, HALF, D), BF16),
            pltpu.VMEM((2, 4, HALF, D), BF16),
            pltpu.VMEM((2, 2, 3, QUART, D), BF16),
            pltpu.VMEM((2, 2, 3, QUART, D), BF16),
            pltpu.VMEM((ROWS, D), BF16),
            pltpu.VMEM((8, ROWS + 8, CH), F32),
            pltpu.VMEM((8, ROWS, CH), F32),
            pltpu.VMEM((8, ROWS, CH), F32),
            pltpu.VMEM((8, ROWS, CH), F32),
            pltpu.VMEM((CH, 2 * CH), BF16),
            pltpu.VMEM((3, 128), F32),
            pltpu.VMEM((8, 128, 128), F32),
            dma((13,)),
            dma((2,)),
            dma((3,)),
            dma((4,)),
            dma((2, 40)),
            dma((2,)),
            dma((2, 10)),
            dma((2,)),
            dma((2, 4)),
            dma((2,)),
            dma((2, 2, 3)),
        ],
        compiler_params=pltpu.CompilerParams(
            collective_id=0, has_side_effects=True, vmem_limit_bytes=62 * 1024 * 1024
        ),
        name="layer",
    )(
        tokens, row(s1), row(s2), row(s3),
        g1.T, u1.T, g3.T, u3.T, ck, decay, inputs, cdw.reshape(3, 128), extra.reshape(8, 128),
        d1, ri, og, mo, d3,
    )


def solution(mesh):
    in_specs = (
        P(("fs", "tp"), None), P(), P("fs", "tp"), P("fs", "tp"), P("tp", "fs"),
        P(), P("fs", "tp"), P("fs", "tp"), P(None, "tp"), P("tp", None, None),
        P("tp", None, None), P("tp"), P("fs"), P("tp", "fs"), P(),
        P("fs", "tp"), P("fs", "tp"), P("tp", "fs"),
    )
    out_specs = P(("fs", "tp"), None)
    return jax.shard_map(shards, mesh=mesh, in_specs=in_specs, out_specs=out_specs, check_vma=False)
```
